256 devices in a mesh: sp: 16 (over y, x), tp: 16 (over z, core).
Axes of the slice: x: 4, y: 4, z: 8, core: 2. Of those that a mesh axis runs over, the one named last changes fastest.
Arguments:
- conv_outer: bfloat16 [2048, 4096], P('tp', 'sp'), may hold values from -6 to 6
- conv_inner: bfloat16 [2048, 4096], P('tp', 'sp'), may hold values from -6 to 6
- conv_input: bfloat16 [2048, 4096], P('tp', 'sp'), may hold values from -6 to 6
- conv_taps: float32 [3, 2048], P(None, 'tp'), may hold values from -3 to 3
- out_proj: bfloat16 [2048, 4096], P('tp'), may hold values from -0.125 to 0.125
- mixed_state: bfloat16 [4096, 4096], P('sp', 'tp'), may hold values from -6 to 6
- route_ids: int32 [4096, 2], P('sp'), may hold values from 0 to 15, all different within a row; in each aligned block of 256 rows (0 to 255, 256 to 511, ...) at most 64 rows name the same one
- route_weights: float32 [4096, 2], P('sp'), may hold values from 0.1 to 1
- w_gate: bfloat16 [16, 2048, 4096], P('sp', 'tp'), may hold values from -0.09375 to 0.09375
- w_up: bfloat16 [16, 2048, 4096], P('sp', 'tp'), may hold values from -0.09375 to 0.09375
- w_down: bfloat16 [16, 2048, 4096], P('sp', 'tp'), may hold values from -0.125 to 0.125
- cotangent: bfloat16 [4096, 4096], P('sp', 'tp'), may hold values from -8 to 8
Outputs:
- grad_gate: float32 [16, 2048, 4096], P('sp', 'tp')
- grad_up: float32 [16, 2048, 4096], P('sp', 'tp')
- grad_down: float32 [16, 2048, 4096], P('sp', 'tp')
- grad_mixed: bfloat16 [4096, 4096], P('sp', 'tp')
- grad_proj: float32 [2048, 4096], P('tp', 'sp')
- grad_outer: bfloat16 [2048, 4096], P('tp', 'sp')
- grad_inner: bfloat16 [2048, 4096], P('tp', 'sp')
- grad_input: bfloat16 [2048, 4096], P('tp', 'sp')
The draws below stay inside these ranges and needn't reach their ends.
Inputs may be any that keep to these rules, and one draw needn't show every extreme that they name: `route_ids`: each row names 2 different experts; among the tokens of one index of sp no expert is named more than 64 times, a bound that some block reaches.
All inputs are finite; a program needn't handle non-finite values.
Results may differ from the reference program's by a relative error of at most 0.022.
Values may be sent and summed in bfloat16 or wider, within the bound.
A program may use at most 128 MiB of HBM per device.

```python
import math
import jax
import jax.numpy as jnp
import numpy as np
from jax import lax

D = 4096
FF = 2048
CH = 2048
TAPS = 3
TOP = 2
TOK_DEV = 256
EXPERTS = 16
CAP = 64
TOKENS = 4096
N_SP = 16
N_TP = 16


def with_spikes(result, rng, source, target, blocks, factor):
    def block_of(dim):
        return (jnp.arange(result.shape[dim]) // (result.shape[dim] // blocks)).reshape((-1,) + (1,) * (result.ndim - 1 - dim))

    near = jax.random.permutation(rng, blocks)[block_of(target)]
    other_side = (block_of(target) + blocks // 2) % blocks
    return jnp.where((block_of(source) == near) | (block_of(source) == other_side), factor * result, result)


def level_of(stream_key, dims, cuts, least, top_value):
    def one(axis_at, shards_of):
        heights = jax.random.uniform(jax.random.fold_in(jax.random.fold_in(stream_key, 6), axis_at), (shards_of,), jnp.float32, least / len(cuts), top_value / len(cuts))
        return jnp.repeat(jnp.exp(heights), dims[axis_at] // shards_of).reshape((-1,) + (1,) * (len(dims) - axis_at - 1))

    factor_of = one(*cuts[0])
    for cut in cuts[1:]:
        factor_of = factor_of * one(*cut)
    return factor_of


def shared_out(stream_key, own, number, rows, amount, top, most, lean):
    ranking = jax.random.permutation(stream_key, amount)
    packed, ordinary = load_shares(amount, rows * top, most, lean, True), load_shares(amount, rows * top, most, lean, False)
    places = jnp.arange(amount)

    def named(lengths, rotation):
        used = int((lengths > 0).sum())
        fixed = max(1, used // 4)
        shifted = fixed + (places - fixed + rotation * (used - fixed)) % max(1, amount - fixed)
        return jnp.zeros((amount,), jnp.int32).at[ranking[jnp.where(places < fixed, places, shifted)]].set(jnp.asarray(lengths, jnp.int32))

    lengths = jnp.where(number % 4 == 0, named(packed, number // 4), named(ordinary, number - number // 4 - 1))
    mixed = jax.random.permutation(jax.random.fold_in(own, 3), amount)
    giver, taker = mixed[0:amount // 2 * 2:2], mixed[1:amount // 2 * 2:2]
    margin = jnp.minimum(lengths[giver] - 1, most - lengths[taker]) // 2
    margin = jnp.where((giver == ranking[0]) | (taker == ranking[0]) | (lengths[taker] == 0), 0, jnp.maximum(margin, 0))
    shifted = jax.random.randint(jax.random.fold_in(own, 4), (amount // 2,), 0, 1 << 20) % (margin + 1)
    lengths = lengths.at[giver].add(-shifted).at[taker].add(shifted)
    items = jnp.searchsorted(jnp.cumsum(lengths), jnp.arange(rows * top), side="right").astype(jnp.int32)
    grid = items.reshape(top, rows).T
    grid = grid[jax.random.permutation(jax.random.fold_in(own, 1), rows)]
    rotation = jax.random.randint(jax.random.fold_in(own, 2), (rows, 1), 0, top)
    return jnp.take_along_axis(grid, (jnp.arange(top)[None, :] + rotation) % top, axis=1)


def load_shares(number_of, total, most, slope, full):
    loads = [(1 << 20) // math.isqrt(standing ** slope) + 1 for standing in range(1, number_of + 1)]
    largest = most if full else min(most, max(-(-total // number_of), total * loads[0] // sum(loads)))
    least = 1 if total - largest >= number_of - 1 else 0
    holding, surplus = [largest] + [least] * (number_of - 1), total - largest - least * (number_of - 1)
    while surplus > 0:
        free = [i for i in range(1, number_of) if holding[i] < largest] or [i for i in range(1, number_of) if holding[i] < most]
        pool, left = sum([loads[i] for i in free]), surplus
        for i in free:
            extra = min(most - holding[i], max(1, left * loads[i] // pool), surplus)
            holding[i] = holding[i] + extra
            surplus = surplus - extra
    return np.array(holding)


def centred(key, extent, scale, limit, split=(), kind=jnp.bfloat16):
    values = jax.random.normal(key, extent, jnp.float32) * scale
    if len(split) > 0:
        values = level_of(key, extent, split, -0.22, 0.18) * values
    return jnp.clip(values, min=-limit, max=limit).astype(kind)


def noise_with(key, shape, spread, most, split, heavy, held_as=jnp.bfloat16):
    drawn = spread * jax.random.normal(key, shape, jnp.float32)
    if split:
        drawn = drawn * level_of(key, shape, split, -0.22, 0.18)
    return jnp.clip(with_spikes(drawn, jax.random.fold_in(key, 3), *heavy), -most, most).astype(held_as)


def setup_inputs(seed: int = 0) -> dict:
    arg_keys = jax.random.split(jax.random.key(seed), 13)
    conv_outer = centred(arg_keys[0], (CH, TOKENS), 1.0, 6.0, ((0, 16), (1, 16)))
    conv_inner = centred(arg_keys[1], (CH, TOKENS), 1.0, 6.0, ((0, 16), (1, 16)))
    conv_input = centred(arg_keys[2], (CH, TOKENS), 1.0, 6.0, ((0, 16), (1, 16)))
    conv_taps = centred(arg_keys[3], (TAPS, CH), 0.6, 3.0, ((1, 16),), jnp.float32)
    out_proj = centred(arg_keys[4], (CH, D), CH ** -0.5, 0.125, ((0, 16),))
    mixed_state = centred(arg_keys[5], (TOKENS, D), 1.0, 6.0, ((0, 16), (1, 16)))
    route_ids_keys = jax.random.split(jax.random.fold_in(arg_keys[6], 1), TOKENS // TOK_DEV)
    route_ids_turns = jax.random.permutation(jax.random.fold_in(arg_keys[6], 3), TOKENS // TOK_DEV)
    route_ids = jax.vmap(lambda own, number: shared_out(jax.random.fold_in(arg_keys[6], 2), own, number, TOK_DEV, EXPERTS, TOP, CAP, 2))(route_ids_keys, route_ids_turns).reshape((TOKENS, TOP))
    route_weights = jnp.clip(0.1 + 0.9 * jax.random.uniform(arg_keys[7], (TOKENS, TOP), jnp.float32) ** level_of(arg_keys[7], (TOKENS, TOP), ((0, 16),), -0.2, 0.2), 0.1, 1.0)
    w_gate = centred(arg_keys[8], (EXPERTS, FF, D), D ** -0.5, 0.09375, ((0, 16), (1, 16)))
    w_up = centred(arg_keys[9], (EXPERTS, FF, D), D ** -0.5, 0.09375, ((0, 16), (1, 16)))
    w_down = centred(arg_keys[10], (EXPERTS, FF, D), FF ** -0.5, 0.125, ((0, 16), (1, 16)))
    cotangent = noise_with(arg_keys[11], (TOKENS, D), 1.0, 8.0, ((0, 16), (1, 16)), (0, 1, 16, 2.0))
    return {"conv_outer": conv_outer, "conv_inner": conv_inner, "conv_input": conv_input, "conv_taps": conv_taps, "out_proj": out_proj, "mixed_state": mixed_state, "route_ids": route_ids, "route_weights": route_weights, "w_gate": w_gate, "w_up": w_up, "w_down": w_down, "cotangent": cotangent}


def expert_core(rows_in, rows_grad, gate_w, up_w, down_w):
    gate_pre = jnp.dot(rows_in, gate_w.T, preferred_element_type=jnp.float32)
    up_pre = jnp.dot(rows_in, up_w.T, preferred_element_type=jnp.float32)
    sig_gate = jax.nn.sigmoid(gate_pre)
    silu_gate = gate_pre * sig_gate
    hidden = (silu_gate * up_pre).astype(jnp.bfloat16)
    back_hidden = jnp.dot(rows_grad, down_w.T, preferred_element_type=jnp.float32)
    back_gate = (back_hidden * up_pre * sig_gate * (1.0 + gate_pre * (1.0 - sig_gate))).astype(jnp.bfloat16)
    back_up = (back_hidden * silu_gate).astype(jnp.bfloat16)
    grad_down_e = jnp.dot(hidden.T, rows_grad, preferred_element_type=jnp.float32)
    grad_gate_e = jnp.dot(back_gate.T, rows_in, preferred_element_type=jnp.float32)
    grad_up_e = jnp.dot(back_up.T, rows_in, preferred_element_type=jnp.float32)
    return back_gate, back_up, grad_gate_e, grad_up_e, grad_down_e


def reference(conv_outer, conv_inner, conv_input, conv_taps, out_proj, mixed_state, route_ids, route_weights, w_gate, w_up, w_down, cotangent):
    block_ids = route_ids.reshape(N_SP, TOP * TOK_DEV)
    onehot = (block_ids[:, :, None] == jnp.arange(EXPERTS, dtype=jnp.int32)[None, None, :]).astype(jnp.int32)
    position = jnp.sum(jnp.cumsum(onehot, axis=1) * onehot, axis=2) - 1
    device_ids = jnp.broadcast_to(jnp.arange(N_SP, dtype=jnp.int32)[:, None], block_ids.shape)
    assign = jnp.arange(N_SP * TOP * TOK_DEV, dtype=jnp.int32).reshape(N_SP, TOP * TOK_DEV)
    table = jnp.full((EXPERTS, N_SP, CAP), -1, jnp.int32).at[block_ids, device_ids, position].set(assign)
    table = table.reshape(EXPERTS, N_SP * CAP)
    weight_flat = route_weights.reshape(-1)

    def expert_pass(operands):
        table_row, gate_w, up_w, down_w = operands
        valid = table_row >= 0
        safe_idx = jnp.where(valid, table_row, 0)
        token_idx = safe_idx // TOP
        rows_in = jnp.where(valid[:, None], mixed_state[token_idx], jnp.zeros((), jnp.bfloat16))
        scale = jnp.where(valid, weight_flat[safe_idx], jnp.zeros((), jnp.float32))
        rows_grad = (cotangent[token_idx].astype(jnp.float32) * scale[:, None]).astype(jnp.bfloat16)
        back_gate, back_up, grad_gate_e, grad_up_e, grad_down_e = expert_core(rows_in, rows_grad, gate_w, up_w, down_w)
        row_count = rows_in.shape[0]
        gate_blocks = back_gate.astype(jnp.float32).reshape(row_count, N_TP, FF // N_TP)
        up_blocks = back_up.astype(jnp.float32).reshape(row_count, N_TP, FF // N_TP)
        gate_wblk = gate_w.astype(jnp.float32).reshape(N_TP, FF // N_TP, D)
        up_wblk = up_w.astype(jnp.float32).reshape(N_TP, FF // N_TP, D)
        partial_value = jnp.einsum("rbf,bfd->brd", gate_blocks, gate_wblk) + jnp.einsum("rbf,bfd->brd", up_blocks, up_wblk)
        rounded = lax.optimization_barrier(partial_value.astype(jnp.bfloat16))
        row_back = jnp.sum(rounded.astype(jnp.float32), axis=0).astype(jnp.bfloat16)
        return row_back, grad_gate_e, grad_up_e, grad_down_e

    row_back, grad_gate, grad_up, grad_down = lax.map(expert_pass, (table, w_gate, w_up, w_down))
    flat_table = table.reshape(-1)
    valid_all = flat_table >= 0
    token_all = jnp.where(valid_all, flat_table, 0) // TOP
    back_vals = jnp.where(valid_all[:, None], row_back.reshape(-1, D).astype(jnp.float32), jnp.zeros((), jnp.float32))
    moe_grad = jnp.zeros((TOKENS, D), jnp.float32).at[token_all].add(back_vals)
    grad_mixed = (cotangent.astype(jnp.float32) + moe_grad).astype(jnp.bfloat16)

    inner_prod = conv_inner.astype(jnp.float32) * conv_input.astype(jnp.float32)
    padded = jnp.pad(inner_prod, ((0, 0), (TAPS - 1, 0)))
    conv_out = jnp.zeros_like(inner_prod)
    for offset in range(TAPS):
        conv_out = conv_out + conv_taps[offset][:, None] * padded[:, offset:offset + TOKENS]
    mixer_act = (conv_outer.astype(jnp.float32) * conv_out).astype(jnp.bfloat16)
    back_mixer = jnp.dot(out_proj, grad_mixed.T, preferred_element_type=jnp.float32)
    grad_proj = jnp.dot(mixer_act, grad_mixed, preferred_element_type=jnp.float32)
    grad_outer = (back_mixer * conv_out).astype(jnp.bfloat16)
    back_conv = back_mixer * conv_outer.astype(jnp.float32)
    padded_back = jnp.pad(back_conv, ((0, 0), (0, TAPS - 1)))
    back_prod = jnp.zeros_like(back_conv)
    for offset in range(TAPS):
        shift_by = TAPS - 1 - offset
        back_prod = back_prod + conv_taps[offset][:, None] * padded_back[:, shift_by:shift_by + TOKENS]
    grad_inner = (back_prod * conv_input.astype(jnp.float32)).astype(jnp.bfloat16)
    grad_input = (back_prod * conv_inner.astype(jnp.float32)).astype(jnp.bfloat16)
    return grad_gate, grad_up, grad_down, grad_mixed, grad_proj, grad_outer, grad_inner, grad_input
```

```python
import functools

import jax
import jax.numpy as jnp
from jax import lax
from jax.experimental import pallas as pl
from jax.experimental.pallas import tpu as pltpu
from jax.sharding import Mesh
from jax.sharding import PartitionSpec as P

BF = jnp.bfloat16
F32 = jnp.float32
MESH_ID = pl.DeviceIdType.MESH
SUBS = 4


def dot(a, b):
    return lax.dot_general(a, b, (((1,), (0,)), ((), ())), preferred_element_type=F32)


def dot_nt(a, b):
    return lax.dot_general(a, b, (((1,), (1,)), ((), ())), preferred_element_type=F32)


def kernel(
    dims,
    ids,
    wts,
    state,
    cot,
    c_outer,
    c_inner,
    c_input,
    taps,
    wg_hbm,
    wu_hbm,
    wd_hbm,
    op_hbm,
    gg_hbm,
    gu_hbm,
    gd_hbm,
    gm_out,
    gproj,
    gouter,
    ginner,
    ginput,
    rows_all,
    wgu,
    wd,
    op,
    sent,
    acc_gu,
    acc_d,
    pick,
    pick_t,
    bgu,
    bgu_t,
    hid_t,
    part_out,
    part_in,
    run,
    back,
    grad_gu,
    grad_d,
    full,
    proj_out,
    proj_in,
    rim_in,
    tail_out,
    tail_in,
    conv_s,
    act_s,
    bm_acc,
    w_sem,
    o_sem,
    a_send,
    a_recv,
    g_send,
    g_recv,
    d_send,
    d_recv,
    p_send,
    p_recv,
    r_send,
    r_recv,
    b_send,
    b_recv,
    f_send,
    f_recv,
    e_send,
    e_recv,
    j_send,
    j_recv,
    h_send,
    h_recv,
    t_send,
    t_recv,
):
    ny, nx, nz = dims
    ns = ny * nx
    hid, d_all = wg_hbm.shape
    toks, feat = state.shape
    cap = sent.shape[2]
    slots = ns * cap
    y, x = lax.axis_index("y"), lax.axis_index("x")
    z, c = lax.axis_index("z"), lax.axis_index("c")
    me = y * nx + x
    other = 1 - c
    up, down = lax.rem(z + 1, nz), lax.rem(z + nz - 1, nz)
    shifts = [(dy, dx) for dy in range(ny) for dx in range(nx) if (dy, dx) != (0, 0)]
    following, previous = lax.rem(me + 1, ns), lax.rem(me + ns - 1, ns)

    def at_plane(dy, dx):
        py, px = lax.rem(y + dy, ny), lax.rem(x + dx, nx)
        return {"y": py, "x": px, "z": z, "c": c}, py * nx + px

    def on_sp(s):
        return {"y": lax.div(s, nx), "x": lax.rem(s, nx), "z": z, "c": c}

    def on_z(pos):
        return {"y": y, "x": x, "z": pos, "c": c}

    partner = {"y": y, "x": x, "z": z, "c": other}

    def remote(src, dst, send, recv, device):
        return pltpu.make_async_remote_copy(
            src_ref=src,
            dst_ref=dst,
            send_sem=send,
            recv_sem=recv,
            device_id=device,
            device_id_type=MESH_ID,
        )

    def cols(index):
        return pl.ds(pl.multiple_of(index * feat, feat), feat)

    loads = [
        pltpu.make_async_copy(wg_hbm, wgu.at[pl.ds(0, hid)], w_sem.at[0]),
        pltpu.make_async_copy(wu_hbm, wgu.at[pl.ds(hid, hid)], w_sem.at[1]),
        pltpu.make_async_copy(wd_hbm, wd, w_sem.at[2]),
        pltpu.make_async_copy(op_hbm, op, w_sem.at[3]),
    ]
    for load in loads:
        load.start()

    barrier = pltpu.get_barrier_semaphore()
    peers = [at_plane(dy, dx)[0] for dy, dx in shifts] + [on_z(up), on_z(down), partner]
    for peer in peers:
        pl.semaphore_signal(barrier, inc=1, device_id=peer, device_id_type=MESH_ID)

    expert = lax.broadcasted_iota(jnp.int32, (ns, toks), 0)
    first, second = ids[0:1, :] == expert, ids[1:2, :] == expert
    named = jnp.where(first, 1.0, 0.0) + jnp.where(second, 1.0, 0.0)
    weight = jnp.where(first, wts[0:1, :], 0.0) + jnp.where(second, wts[1:2, :], 0.0)
    earlier = jnp.where(
        lax.broadcasted_iota(jnp.int32, (toks, toks), 0)
        < lax.broadcasted_iota(jnp.int32, (toks, toks), 1),
        1.0,
        0.0,
    ).astype(BF)
    count = jnp.where(named > 0.0, dot(named.astype(BF), earlier), -1.0)
    place = lax.broadcasted_iota(jnp.int32, (cap, toks), 0).astype(F32)
    scales = []
    for e in range(ns):
        hit = jnp.where(count[e : e + 1, :] == place, 1.0, 0.0)
        pick[pl.ds(e * cap, cap), :] = hit.astype(BF)
        scales.append(jnp.sum(hit * weight[e : e + 1, :], axis=1, keepdims=True))
    scale = jnp.concatenate(scales, axis=0)
    sent[0] = dot(pick[...], state[...]).astype(BF).reshape(ns, cap, feat)
    sent[1] = (dot(pick[...], cot[...]) * scale).astype(BF).reshape(ns, cap, feat)

    pl.semaphore_wait(barrier, len(peers))

    def route_copy(arr, index, dst_z, dev, s_to):
        return remote(
            sent.at[arr, s_to],
            rows_all.at[arr, z, c, me],
            a_send.at[arr, index],
            a_recv.at[arr, me],
            dev,
        )

    def route_wait(arr, s_from):
        remote(
            sent.at[arr, s_from],
            rows_all.at[arr, z, c, s_from],
            a_send.at[arr, 0],
            a_recv.at[arr, s_from],
            partner,
        ).wait_recv()

    for index, (dy, dx) in enumerate(shifts):
        dev, s_to = at_plane(dy, dx)
        for arr in range(2):
            route_copy(arr, index, z, dev, s_to).start()
    for arr in range(2):
        rows_all[arr, z, c, me] = sent[arr, me]

    def rim_copy(arr, dev):
        src = (c_inner, c_input)[arr]
        lanes = src.shape[1]
        return remote(
            src.at[:, pl.ds(lanes - 128, 128)], rim_in.at[arr], h_send.at[arr], h_recv.at[arr], dev
        )

    for arr in range(2):
        rim_copy(arr, on_sp(following)).start()

    acc_gu[...] = jnp.zeros_like(acc_gu)
    acc_d[...] = jnp.zeros_like(acc_d)
    per_sub = ns // SUBS

    def source_of(arr, t):
        return lax.rem(z + nz - t, nz) if arr == 0 else lax.rem(z + t, nz)

    def ring_copy(arr, sub, t):
        part = rows_all.at[arr, source_of(arr, t), c, pl.ds(sub * per_sub, per_sub)]
        return remote(
            part,
            part,
            g_send.at[arr, sub, t],
            g_recv.at[arr, sub, t],
            on_z(up if arr == 0 else down),
        )

    def ring_wait(arr, sub, t):
        part = rows_all.at[arr, source_of(arr, t), c, pl.ds(sub * per_sub, per_sub)]
        remote(
            part, part, g_send.at[arr, sub, t - 1], g_recv.at[arr, sub, t - 1], partner
        ).wait_recv()

    def share(arr, t):
        part = rows_all.at[arr, source_of(arr, t), c]
        return remote(part, part, d_send.at[arr, t], d_recv.at[arr, t], partner)

    def share_wait(arr, t):
        part = rows_all.at[arr, source_of(arr, t), other]
        remote(part, part, d_send.at[arr, t], d_recv.at[arr, t], partner).wait_recv()

    def products(t):
        for arr in range(2):
            share_wait(arr, t)
        for lane in range(2):
            at = source_of(0, t)
            rows = rows_all[0, at, lane].reshape(slots, feat)
            acc_gu[...] += dot_nt(rows, wgu[:, cols(at * 2 + lane)])
            at = source_of(1, t)
            rows = rows_all[1, at, lane].reshape(slots, feat)
            acc_d[...] += dot_nt(rows, wd[:, cols(at * 2 + lane)])

    for sub in range(SUBS):
        for arr in range(2):
            for s_from in range(sub * per_sub, (sub + 1) * per_sub):

                @pl.when(s_from != me)
                def _():
                    route_wait(arr, s_from)

            ring_copy(arr, sub, 0).start()
    for arr in range(2):
        share(arr, 0).start()

    for arr in range(2):
        rim_copy(arr, on_sp(previous)).wait_recv()
    inner, inp = c_inner[...].astype(F32), c_input[...].astype(F32)
    rim_prod = rim_in[0].astype(F32) * rim_in[1].astype(F32)
    rim_prod = jnp.where(me == 0, 0.0, rim_prod)
    ext = jnp.concatenate([rim_prod, inner * inp], axis=1)
    n_taps = taps.shape[1]
    conv_out = taps[:, n_taps - 1 : n_taps] * (inner * inp)
    for j in range(n_taps - 1):
        conv_out = conv_out + taps[:, j : j + 1] * pltpu.roll(ext, n_taps - 1 - j, 1)[:, 128:]
    conv_s[...] = conv_out
    act_s[...] = (c_outer[...].astype(F32) * conv_out).astype(BF)
    pick_t[...] = pick[...].T

    for load in loads:
        load.wait()

    def ring_step(t, carry):
        for sub in range(SUBS):
            for arr in range(2):
                ring_wait(arr, sub, t)

                @pl.when(t < nz - 1)
                def _():
                    ring_copy(arr, sub, t).start()

        for arr in range(2):
            share(arr, t).start()
        products(t - 1)
        return carry

    lax.fori_loop(1, nz, ring_step, 0)
    products(nz - 1)

    gate_pre, up_pre = acc_gu[:, :hid], acc_gu[:, hid:]
    back_hidden = acc_d[...]
    sig = jax.nn.sigmoid(gate_pre)
    silu = gate_pre * sig
    hid_t[...] = (silu * up_pre).astype(BF).T
    back_gate = (back_hidden * up_pre * sig * (1.0 + gate_pre * (1.0 - sig))).astype(BF)
    back_up = (back_hidden * silu).astype(BF)
    bgu[:, :hid] = back_gate
    bgu[:, hid:] = back_up
    bgu_t[:hid, :] = back_gate.T
    bgu_t[hid:, :] = back_up.T

    half = slots // 2
    quarter = half // 2

    def target_of(way, t):
        return lax.rem(z + 2 * nz - 1 - t, nz) if way == 0 else lax.rem(z + 1 + t, nz)

    def part_copy(way, t):
        return remote(
            part_out.at[way, t], part_in.at[way, t], p_send.at[way, t], p_recv.at[way, t], partner
        )

    def partner_part(t):
        for way in range(2):
            w = wgu[:, cols(target_of(way, t) * 2 + other)]
            part_out[way, t] = dot(bgu[pl.ds(way * half, half), :], w).astype(BF)
            part_copy(way, t).start()

    def run_copy(way, sub, t):
        rows = pl.ds(sub * quarter, quarter)
        return remote(
            run.at[way, t, rows],
            run.at[way, t + 1, rows],
            r_send.at[way, sub, t],
            r_recv.at[way, sub, t],
            on_z(up if way == 0 else down),
        )

    for way in range(2):
        run[way, 0] = jnp.zeros((half, feat), BF)
    partner_part(0)

    def reduce_step(t, carry):
        @pl.when(t < nz - 1)
        def _():
            partner_part(t + 1)

        for lane in range(2):
            rows = rows_all[0, t, lane].reshape(slots, feat)
            grad_gu[:, cols(t * 2 + lane)] = dot(bgu_t[...], rows)
            rows = rows_all[1, t, lane].reshape(slots, feat)
            grad_d[:, cols(t * 2 + lane)] = dot(hid_t[...], rows)
        for way in range(2):
            part_copy(way, t).wait_recv()
        for sub in range(2):
            for way in range(2):
                rows = pl.ds(sub * quarter, quarter)

                @pl.when(t > 0)
                def _():
                    run_copy(way, sub, t - 1).wait_recv()

                w = wgu[:, cols(target_of(way, t) * 2 + c)]
                own = dot(bgu[pl.ds(way * half + sub * quarter, quarter), :], w)
                total = own + part_in[way, t, rows].astype(F32) + run[way, t, rows].astype(F32)
                run[way, t, rows] = total.astype(BF)

                @pl.when(t < nz - 1)
                def _():
                    run_copy(way, sub, t).start()

        return carry

    lax.fori_loop(0, nz, reduce_step, 0)

    results = [
        pltpu.make_async_copy(grad_gu.at[pl.ds(0, hid)], gg_hbm, o_sem.at[0]),
        pltpu.make_async_copy(grad_gu.at[pl.ds(hid, hid)], gu_hbm, o_sem.at[1]),
        pltpu.make_async_copy(grad_d, gd_hbm, o_sem.at[2]),
    ]

    def back_src(s):
        way, row = lax.div(s, ns // 2), lax.rem(s, ns // 2)
        return run.at[way, nz - 1, pl.ds(pl.multiple_of(row * cap, cap), cap)]

    def back_copy(index, dev, s_to):
        return remote(back_src(s_to), back.at[me], b_send.at[index], b_recv.at[me], dev)

    for index, (dy, dx) in enumerate(shifts):
        dev, s_to = at_plane(dy, dx)
        back_copy(index, dev, s_to).start()
    back[me] = back_src(me)[...]
    for result in results:
        result.start()
    for dy, dx in shifts:
        _, s_from = at_plane(dy, dx)
        remote(
            back_src(s_from), back.at[s_from], b_send.at[0], b_recv.at[s_from], partner
        ).wait_recv()
    moe = dot(pick_t[...], back[...].reshape(slots, feat))
    grad_mixed = (cot[...].astype(F32) + moe).astype(BF)
    gm_out[...] = grad_mixed
    full[z, c] = grad_mixed

    halves = toks // 2
    hops = {(0, h): nz // 2 - h for h in range(2)} | {(1, h): nz // 2 - 1 + h for h in range(2)}

    def full_part(way, h, k, lane):
        at = lax.rem(z + nz - k, nz) if way == 0 else lax.rem(z + k, nz)
        return full.at[at, lane, pl.ds(h * halves, halves)]

    def full_copy(way, h, k):
        part = full_part(way, h, k, c)
        return remote(
            part, part, f_send.at[way, h, k], f_recv.at[way, h, k], on_z(up if way == 0 else down)
        )

    def full_wait(way, h, k):
        part = full_part(way, h, k, c)
        remote(
            part, part, f_send.at[way, h, k - 1], f_recv.at[way, h, k - 1], partner
        ).wait_recv()

    def full_share(way, h, k, lane):
        part = full_part(way, h, k, lane)
        return remote(part, part, e_send.at[way, h, k], e_recv.at[way, h, k], partner)

    bm_acc[...] = jnp.zeros_like(bm_acc)

    def mixer_products(at):
        for lane in range(2):
            f = full[at, lane]
            bm_acc[...] += dot_nt(op[:, cols(at * 2 + lane)], f)
            proj_out[at * 2 + lane] = dot(act_s[...], f).astype(BF)

    shared = []
    for h in range(2):
        for way in range(2):
            if hops[(way, h)] > 0:
                full_copy(way, h, 0).start()
    for h in range(2):
        full_share(0, h, 0, c).start()
        shared.append((0, h, 0))
    pending = [(0, [(0, 0, 0), (0, 1, 0)])]
    for k in range(1, nz // 2 + 1):
        news = {}
        for h in range(2):
            for way in range(2):
                if k > hops[(way, h)]:
                    continue
                full_wait(way, h, k)
                if k < hops[(way, h)]:
                    full_copy(way, h, k).start()
                full_share(way, h, k, c).start()
                shared.append((way, h, k))
                news.setdefault(k if (way == 0 or 2 * k == nz) else -k, []).append((way, h, k))
        for pos, waits in pending:
            for args in waits:
                full_share(*args, other).wait_recv()
            mixer_products(lax.rem(z + nz - pos, nz))
        pending = list(news.items())
    for pos, waits in pending:
        for args in waits:
            full_share(*args, other).wait_recv()
        mixer_products(lax.rem(z + nz - pos, nz))

    back_mixer = bm_acc[...]
    back_conv = back_mixer * c_outer[...].astype(F32)
    tail_out[...] = back_conv[:, :128]

    def tail_copy(dev):
        return remote(tail_out, tail_in, t_send.at[0], t_recv.at[0], dev)

    tail_copy(on_sp(previous)).start()

    def proj_copy(index, dev, s_to):
        return remote(proj_out.at[s_to], proj_in.at[me], j_send.at[index], j_recv.at[me], dev)

    for index, (dy, dx) in enumerate(shifts):
        dev, s_to = at_plane(dy, dx)
        proj_copy(index, dev, s_to).start()

    gouter[...] = (back_mixer * conv_s[...]).astype(BF)
    tail_copy(on_sp(following)).wait_recv()
    tail = jnp.where(me == ns - 1, 0.0, tail_in[...])
    ext = jnp.concatenate([back_conv, tail], axis=1)
    width = ext.shape[1]
    back_prod = taps[:, n_taps - 1 : n_taps] * back_conv
    for j in range(n_taps - 1):
        back_prod = (
            back_prod + taps[:, j : j + 1] * pltpu.roll(ext, width - (n_taps - 1 - j), 1)[:, :toks]
        )
    ginner[...] = (back_prod * c_input[...].astype(F32)).astype(BF)
    ginput[...] = (back_prod * c_inner[...].astype(F32)).astype(BF)

    proj_total = proj_out[me].astype(F32)
    for dy, dx in shifts:
        _, s_from = at_plane(dy, dx)
        remote(
            proj_out.at[s_from], proj_in.at[s_from], j_send.at[0], j_recv.at[s_from], partner
        ).wait_recv()
        proj_total = proj_total + proj_in[s_from].astype(F32)
    gproj[...] = proj_total

    for result in results:
        result.wait()
    for index, (dy, dx) in enumerate(shifts):
        dev, s_to = at_plane(dy, dx)
        for arr in range(2):
            route_copy(arr, index, z, dev, s_to).wait_send()
        back_copy(index, dev, s_to).wait_send()
        proj_copy(index, dev, s_to).wait_send()
    for arr in range(2):
        rim_copy(arr, on_sp(following)).wait_send()
    tail_copy(on_sp(previous)).wait_send()

    def ring_sent(t, carry):
        for arr in range(2):
            for sub in range(SUBS):
                ring_copy(arr, sub, t).wait_send()
            for sub in range(2):
                run_copy(arr, sub, t).wait_send()
        return carry

    lax.fori_loop(0, nz - 1, ring_sent, 0)

    def shares_sent(t, carry):
        for arr in range(2):
            share(arr, t).wait_send()
            part_copy(arr, t).wait_send()
        return carry

    lax.fori_loop(0, nz, shares_sent, 0)
    for (way, h), n in hops.items():
        for k in range(n):
            full_copy(way, h, k).wait_send()
    for args in shared:
        full_share(*args, c).wait_send()


def shards(
    dims,
    conv_outer,
    conv_inner,
    conv_input,
    conv_taps,
    out_proj,
    mixed_state,
    route_ids,
    route_weights,
    w_gate,
    w_up,
    w_down,
    cotangent,
):
    ny, nx, nz = dims
    ns = ny * nx
    toks, feat = mixed_state.shape
    hid, d_all = out_proj.shape[0], out_proj.shape[1]
    chans = conv_outer.shape[0]
    hid = w_gate.shape[1]
    cap = 4 * toks // ns
    slots = ns * cap
    vmem = pl.BlockSpec(memory_space=pltpu.VMEM)
    hbm = pl.BlockSpec(memory_space=pl.ANY)
    dma = pltpu.SemaphoreType.DMA
    scratch = [
        pltpu.VMEM((2, nz, 2, ns, cap, feat), BF),
        pltpu.VMEM((2 * hid, d_all), BF),
        pltpu.VMEM((hid, d_all), BF),
        pltpu.VMEM((chans, d_all), BF),
        pltpu.VMEM((2, ns, cap, feat), BF),
        pltpu.VMEM((slots, 2 * hid), F32),
        pltpu.VMEM((slots, hid), F32),
        pltpu.VMEM((slots, toks), BF),
        pltpu.VMEM((toks, slots), BF),
        pltpu.VMEM((slots, 2 * hid), BF),
        pltpu.VMEM((2 * hid, slots), BF),
        pltpu.VMEM((hid, slots), BF),
        pltpu.VMEM((2, nz, slots // 2, feat), BF),
        pltpu.VMEM((2, nz, slots // 2, feat), BF),
        pltpu.VMEM((2, nz, slots // 2, feat), BF),
        pltpu.VMEM((ns, cap, feat), BF),
        pltpu.VMEM((2 * hid, d_all), F32),
        pltpu.VMEM((hid, d_all), F32),
        pltpu.VMEM((nz, 2, toks, feat), BF),
        pltpu.VMEM((nz * 2, chans, feat), BF),
        pltpu.VMEM((ns, chans, feat), BF),
        pltpu.VMEM((2, chans, 128), BF),
        pltpu.VMEM((chans, 128), F32),
        pltpu.VMEM((chans, 128), F32),
        pltpu.VMEM((chans, toks), F32),
        pltpu.VMEM((chans, toks), BF),
        pltpu.VMEM((chans, toks), F32),
        dma((4,)),
        dma((3,)),
        dma((2, ns)),
        dma((2, ns)),
        dma((2, SUBS, nz)),
        dma((2, SUBS, nz)),
        dma((2, nz)),
        dma((2, nz)),
        dma((2, nz)),
        dma((2, nz)),
        dma((2, 2, nz)),
        dma((2, 2, nz)),
        dma((ns,)),
        dma((ns,)),
        dma((2, 2, nz)),
        dma((2, 2, nz)),
        dma((2, 2, nz)),
        dma((2, 2, nz)),
        dma((ns,)),
        dma((ns,)),
        dma((2,)),
        dma((2,)),
        dma((1,)),
        dma((1,)),
    ]
    grad = jax.ShapeDtypeStruct((hid, d_all), F32)
    conv = jax.ShapeDtypeStruct((chans, toks), BF)
    outs = pl.pallas_call(
        functools.partial(kernel, dims),
        out_shape=(
            grad,
            grad,
            grad,
            jax.ShapeDtypeStruct((toks, feat), BF),
            jax.ShapeDtypeStruct((chans, feat), F32),
            conv,
            conv,
            conv,
        ),
        in_specs=[vmem] * 8 + [hbm] * 4,
        out_specs=(hbm,) * 3 + (vmem,) * 5,
        scratch_shapes=scratch,
        compiler_params=pltpu.CompilerParams(
            collective_id=0, has_side_effects=True, vmem_limit_bytes=66000000
        ),
    )(
        route_ids.T,
        route_weights.T,
        mixed_state,
        cotangent,
        conv_outer,
        conv_inner,
        conv_input,
        conv_taps.T,
        w_gate[0],
        w_up[0],
        w_down[0],
        out_proj,
    )
    return (outs[0][None], outs[1][None], outs[2][None], *outs[3:])


def solution(mesh):
    dims = (4, 4, 8)
    return on_torus(Mesh(mesh.devices.reshape(*dims, 2), ("y", "x", "z", "c")), dims)


def on_torus(torus, dims):
    sp, tp = ("y", "x"), ("z", "c")
    return jax.shard_map(
        functools.partial(shards, dims),
        mesh=torus,
        in_specs=(
            P(tp, sp),
            P(tp, sp),
            P(tp, sp),
            P(None, tp),
            P(tp, None),
            P(sp, tp),
            P(sp, None),
            P(sp, None),
            P(sp, tp, None),
            P(sp, tp, None),
            P(sp, tp, None),
            P(sp, tp),
        ),
        out_specs=(
            P(sp, tp, None),
            P(sp, tp, None),
            P(sp, tp, None),
            P(sp, tp),
            P(tp, sp),
            P(tp, sp),
            P(tp, sp),
            P(tp, sp),
        ),
        check_vma=False,
    )
```

```python
import functools

import jax
import jax.numpy as jnp
from jax import lax
from jax.experimental import pallas as pl
from jax.experimental.pallas import tpu as pltpu
from jax.sharding import Mesh
from jax.sharding import PartitionSpec as P

BF = jnp.bfloat16
F32 = jnp.float32
MESH_ID = pl.DeviceIdType.MESH
SUBS = 2
PIECES = 4


def dot(a, b):
    return lax.dot_general(a, b, (((1,), (0,)), ((), ())), preferred_element_type=F32)


def dot_nt(a, b):
    return lax.dot_general(a, b, (((1,), (1,)), ((), ())), preferred_element_type=F32)


def kernel(
    dims,
    ids,
    wts,
    state,
    cot,
    c_outer,
    c_inner,
    c_input,
    taps,
    wg_hbm,
    wu_hbm,
    wd_hbm,
    op_hbm,
    gg_hbm,
    gu_hbm,
    gd_hbm,
    gm_out,
    gproj,
    gouter,
    ginner,
    ginput,
    rows_all,
    wgu,
    wd,
    op,
    sent,
    raw,
    routed,
    acc_gu,
    acc_d,
    pick,
    pick_t,
    bgu,
    bgu_t,
    hid_t,
    part_out,
    part_in,
    run,
    own_s,
    back,
    side_out,
    side_in,
    group_out,
    group_in,
    far_out,
    far_in,
    grad_gu,
    grad_d,
    full,
    proj_out,
    proj_in,
    rim_in,
    tail_out,
    tail_in,
    conv_s,
    act_s,
    bm_acc,
    w_sem,
    o_sem,
    a_send,
    a_recv,
    g_send,
    g_recv,
    d_send,
    d_recv,
    c_send,
    c_recv,
    q_send,
    q_recv,
    s_send,
    s_recv,
    p_send,
    p_recv,
    r_send,
    r_recv,
    b_send,
    b_recv,
    f_send,
    f_recv,
    e_send,
    e_recv,
    j_send,
    j_recv,
    h_send,
    h_recv,
    t_send,
    t_recv,
    u_send,
    u_recv,
    v_send,
    v_recv,
    y_send,
    y_recv,
):
    ny, nx, nz = dims
    ns = ny * nx
    hid, d_all = wg_hbm.shape
    toks, feat = state.shape
    cap = sent.shape[1]
    slots = ns * cap
    y, x = lax.axis_index("y"), lax.axis_index("x")
    z, c = lax.axis_index("z"), lax.axis_index("c")
    me = y * nx + x
    other = 1 - c
    up, down = lax.rem(z + 1, nz), lax.rem(z + nz - 1, nz)
    shifts = [(dy, dx) for dy in range(ny) for dx in range(nx) if (dy, dx) != (0, 0)]
    following, previous = lax.rem(me + 1, ns), lax.rem(me + ns - 1, ns)

    def at_plane(dy, dx):
        py, px = lax.rem(y + dy, ny), lax.rem(x + dx, nx)
        return {"y": py, "x": px, "z": z, "c": c}, py * nx + px

    def on_sp(s):
        return {"y": lax.div(s, nx), "x": lax.rem(s, nx), "z": z, "c": c}

    def on_z(pos):
        return {"y": y, "x": x, "z": pos, "c": c}

    partner = {"y": y, "x": x, "z": z, "c": other}

    def remote(src, dst, send, recv, device):
        return pltpu.make_async_remote_copy(
            src_ref=src,
            dst_ref=dst,
            send_sem=send,
            recv_sem=recv,
            device_id=device,
            device_id_type=MESH_ID,
        )

    def half_cols(index, off):
        return pl.ds(pl.multiple_of(index * feat + off, feat // 2), feat // 2)

    def cols(index):
        return pl.ds(pl.multiple_of(index * feat, feat), feat)

    loads = [
        pltpu.make_async_copy(wg_hbm, wgu.at[pl.ds(0, hid)], w_sem.at[0]),
        pltpu.make_async_copy(wu_hbm, wgu.at[pl.ds(hid, hid)], w_sem.at[1]),
        pltpu.make_async_copy(wd_hbm, wd, w_sem.at[2]),
        pltpu.make_async_copy(op_hbm, op, w_sem.at[3]),
    ]
    for load in loads:
        load.start()

    barrier = pltpu.get_barrier_semaphore()
    peers = [at_plane(dy, dx)[0] for dy, dx in shifts] + [partner]
    peers += [on_z(lax.rem(z + step, nz)) for step in range(1, nz)]
    for peer in peers:
        pl.semaphore_signal(barrier, inc=1, device_id=peer, device_id_type=MESH_ID)

    pl.semaphore_wait(barrier, len(peers))

    halves = toks // 2
    hops = {(0, h): nz // 2 - h for h in range(2)} | {(1, h): nz // 2 - 1 + h for h in range(2)}

    def along(way, k):
        return lax.rem(z + nz - k, nz) if way == 0 else lax.rem(z + k, nz)

    def raw_copy(way, h, k):
        rows = pl.ds(h * halves, halves)
        src = cot.at[rows] if k == 0 else raw.at[along(way, k), rows]
        return remote(
            src,
            raw.at[along(way, k), rows],
            c_send.at[way, h, k],
            c_recv.at[way, h, k],
            on_z(up if way == 0 else down),
        )

    def raw_wait(way, h, k):
        part = raw.at[along(way, k), pl.ds(h * halves, halves)]
        remote(
            part, part, c_send.at[way, h, k - 1], c_recv.at[way, h, k - 1], partner
        ).wait_recv()

    for h in range(2):
        for way in range(2):
            if hops[(way, h)] > 0:
                raw_copy(way, h, 0).start()

    expert = lax.broadcasted_iota(jnp.int32, (ns, toks), 0)
    first, second = ids[0:1, :] == expert, ids[1:2, :] == expert
    named = jnp.where(first, 1.0, 0.0) + jnp.where(second, 1.0, 0.0)
    weight = jnp.where(first, wts[0:1, :], 0.0) + jnp.where(second, wts[1:2, :], 0.0)
    earlier = jnp.where(
        lax.broadcasted_iota(jnp.int32, (toks, toks), 0)
        < lax.broadcasted_iota(jnp.int32, (toks, toks), 1),
        1.0,
        0.0,
    ).astype(BF)
    count = jnp.where(named > 0.0, dot(named.astype(BF), earlier), -1.0)
    place = lax.broadcasted_iota(jnp.int32, (cap, toks), 0).astype(F32)
    scales = []
    for e in range(ns):
        hit = jnp.where(count[e : e + 1, :] == place, 1.0, 0.0)
        pick[pl.ds(e * cap, cap), :] = hit.astype(BF)
        scales.append(jnp.sum(hit * weight[e : e + 1, :], axis=1, keepdims=True))
    scale = jnp.concatenate(scales, axis=0)
    sent[...] = dot(pick[...], state[...]).astype(BF).reshape(ns, cap, feat)

    def route_copy(index, dev, s_to):
        return remote(
            sent.at[s_to], rows_all.at[0, z, c, me], a_send.at[index], a_recv.at[me], dev
        )

    def route_wait(s_from):
        part = rows_all.at[0, z, c, s_from]
        remote(part, part, a_send.at[0], a_recv.at[s_from], partner).wait_recv()

    for index, (dy, dx) in enumerate(shifts):
        dev, s_to = at_plane(dy, dx)
        route_copy(index, dev, s_to).start()
    rows_all[0, z, c, me] = sent[me]

    def rim_copy(arr, dev):
        src = (c_inner, c_input)[arr]
        lanes = src.shape[1]
        return remote(
            src.at[:, pl.ds(lanes - 128, 128)], rim_in.at[arr], h_send.at[arr], h_recv.at[arr], dev
        )

    for arr in range(2):
        rim_copy(arr, on_sp(following)).start()

    def z_of(i):
        step = lax.div(i + 1, 2)
        return lax.rem(z + nz + step * (1 - 2 * lax.rem(i, 2)), nz)

    def cot_copy(i, index, dev, s_to):
        return remote(
            routed.at[i, s_to],
            rows_all.at[1, z_of(i), c, me],
            q_send.at[i, index],
            q_recv.at[i, me],
            dev,
        )

    def cot_wait(i, s_from):
        part = rows_all.at[1, z_of(i), c, s_from]
        remote(part, part, q_send.at[i, 0], q_recv.at[i, s_from], partner).wait_recv()

    def cot_route(i, rows):
        picked = dot(pick[...], rows) * scale
        routed[i] = picked.astype(BF).reshape(ns, cap, feat)
        for index, (dy, dx) in enumerate(shifts):
            dev, s_to = at_plane(dy, dx)
            cot_copy(i, index, dev, s_to).start()
        rows_all[1, z_of(i), c, me] = routed[i, me]

    acc_gu[...] = jnp.zeros_like(acc_gu)
    acc_d[...] = jnp.zeros_like(acc_d)
    half = slots // 2
    ring_s = ns // 2
    per_sub = ring_s // SUBS

    def ring_copy(way, sub, t):
        part = rows_all.at[0, along(way, t), c, pl.ds(way * ring_s + sub * per_sub, per_sub)]
        return remote(
            part,
            part,
            g_send.at[way, sub, t],
            g_recv.at[way, sub, t],
            on_z(up if way == 0 else down),
        )

    def ring_wait(way, sub, t):
        part = rows_all.at[0, along(way, t), c, pl.ds(way * ring_s + sub * per_sub, per_sub)]
        remote(
            part, part, g_send.at[way, sub, t - 1], g_recv.at[way, sub, t - 1], partner
        ).wait_recv()

    def share(way, t, lane):
        part = rows_all.at[0, along(way, t), lane, pl.ds(way * ring_s, ring_s)]
        return remote(part, part, d_send.at[way, t], d_recv.at[way, t], partner)

    def cot_share(i, lane):
        part = rows_all.at[1, z_of(i), lane]
        return remote(part, part, s_send.at[i], s_recv.at[i], partner)

    def state_products(t):
        for way in range(2):
            share(way, t, other).wait_recv()
        for way in range(2):
            at = along(way, t)
            for lane in range(2):
                rows = rows_all[0, at, lane, way * ring_s : (way + 1) * ring_s]
                acc_gu[way * half : (way + 1) * half, :] += dot_nt(
                    rows.reshape(half, feat), wgu[:, cols(at * 2 + lane)]
                )

    def cot_products(i):
        cot_share(i, other).wait_recv()
        for lane in range(2):
            rows = rows_all[1, z_of(i), lane].reshape(slots, feat)
            acc_d[...] += dot_nt(rows, wd[:, cols(z_of(i) * 2 + lane)])

    def cot_arrived(i):
        for dy, dx in shifts:
            cot_wait(i, at_plane(dy, dx)[1])
        cot_share(i, c).start()

    cot_route(0, cot[...])
    for sub in range(SUBS):
        for way in range(2):
            first_s = way * ring_s + sub * per_sub
            for s_from in range(first_s, first_s + per_sub):

                @pl.when(s_from != me)
                def _():
                    route_wait(s_from)

            ring_copy(way, sub, 0).start()
    for way in range(2):
        share(way, 0, c).start()
    for load in loads:
        load.wait()

    def ring_step(t):
        for sub in range(SUBS):
            for way in range(2):
                ring_wait(way, sub, t)

                @pl.when(t < nz - 1)
                def _():
                    ring_copy(way, sub, t).start()

        for way in range(2):
            share(way, t, c).start()

    for k in range(1, nz // 2 + 1):
        for h in range(2):
            for way in range(2):
                if k <= hops[(way, h)]:
                    raw_wait(way, h, k)
                    if k < hops[(way, h)]:
                        raw_copy(way, h, k).start()
        cot_route(2 * k - 1, raw[along(0, k)])
        if 2 * k < nz:
            cot_route(2 * k, raw[along(1, k)])

    for arr in range(2):
        rim_copy(arr, on_sp(previous)).wait_recv()
    inner, inp = c_inner[...].astype(F32), c_input[...].astype(F32)
    rim_prod = rim_in[0].astype(F32) * rim_in[1].astype(F32)
    rim_prod = jnp.where(me == 0, 0.0, rim_prod)
    ext = jnp.concatenate([rim_prod, inner * inp], axis=1)
    n_taps, chans = taps.shape
    diagonal = lax.broadcasted_iota(jnp.int32, (chans, chans), 0) == lax.broadcasted_iota(
        jnp.int32, (chans, chans), 1
    )
    tap = [
        jnp.sum(jnp.where(diagonal, taps[j : j + 1, :], 0.0), axis=1, keepdims=True)
        for j in range(n_taps)
    ]
    conv_out = tap[n_taps - 1] * (inner * inp)
    for j in range(n_taps - 1):
        conv_out = conv_out + tap[j] * pltpu.roll(ext, n_taps - 1 - j, 1)[:, 128:]
    conv_s[...] = conv_out
    act_s[...] = (c_outer[...].astype(F32) * conv_out).astype(BF)
    pick_t[...] = pick[...].T

    def gather_step(t, carry):
        ring_step(t)
        cot_arrived(t - 1)
        state_products(t - 1)

        @pl.when(t > 1)
        def _():
            cot_products(t - 2)

        return carry

    lax.fori_loop(1, nz, gather_step, 0)
    cot_arrived(nz - 1)
    state_products(nz - 1)
    if nz > 1:
        cot_products(nz - 2)
    cot_products(nz - 1)

    gate_pre, up_pre = acc_gu[:, :hid], acc_gu[:, hid:]
    back_hidden = acc_d[...]
    sig = jax.nn.sigmoid(gate_pre)
    silu = gate_pre * sig
    hid_t[...] = (silu * up_pre).astype(BF).T
    back_gate = (back_hidden * up_pre * sig * (1.0 + gate_pre * (1.0 - sig))).astype(BF)
    back_up = (back_hidden * silu).astype(BF)
    bgu[:, :hid] = back_gate
    bgu[:, hid:] = back_up
    bgu_t[:hid, :] = back_gate.T
    bgu_t[hid:, :] = back_up.T

    quarter = half // 2

    def target_of(way, t):
        return lax.rem(z + 2 * nz - 1 - t, nz) if way == 0 else lax.rem(z + 1 + t, nz)

    def part_copy(way, t):
        return remote(
            part_out.at[way, t], part_in.at[way, t], p_send.at[way, t], p_recv.at[way, t], partner
        )

    def partner_part(t):
        for way in range(2):
            w = wgu[:, half_cols(target_of(way, t) * 2 + other, 0)]
            part_out[way, t] = dot(bgu[pl.ds(way * half, half), :], w).astype(BF)
            part_copy(way, t).start()

    n_groups = nz // 2
    narrow = feat // 2

    def z_of_side(j):
        return lax.rem(lax.div(z, 2) + 1 + lax.div(j, 2), n_groups) * 2 + lax.rem(j, 2)

    def side_copy(j):
        return remote(side_out.at[j], side_in.at[j], u_send.at[j], u_recv.at[j], partner)

    def side_part(j, carry):
        w = wgu[:, half_cols(z_of_side(j) * 2 + other, narrow)]
        side_out[j] = dot(bgu[...], w).astype(BF)
        side_copy(j).start()
        return carry

    def group_copy(g, index, dev, s_to):
        return remote(
            group_out.at[g, s_to], group_in.at[g, me], v_send.at[g, index], v_recv.at[g, me], dev
        )

    def send_group(g):
        for lane in range(2):
            j = 2 * g + lane
            side_copy(j).wait_recv()
            w = wgu[:, half_cols(z_of_side(j) * 2 + c, narrow)]
            total = dot(bgu[...], w) + side_in[j].astype(F32)
            group_out[g, :, :, lane * narrow : (lane + 1) * narrow] = total.astype(BF).reshape(
                ns, cap, narrow
            )
        for index, (dy, dx) in enumerate(shifts):
            dev, s_to = at_plane(dy, dx)
            group_copy(g, index, dev, s_to).start()
        group_in[g, me] = group_out[g, me]

    def far_copy(at):
        return remote(far_out.at[at], far_in.at[z], y_send.at[at], y_recv.at[z], on_z(at))

    def take_group(g):
        for dy, dx in shifts:
            s_from = at_plane(dy, dx)[1]
            part = group_in.at[g, s_from]
            remote(part, part, v_send.at[g, 0], v_recv.at[g, s_from], partner).wait_recv()
        moved = dot(pick_t[...], group_in[g].reshape(slots, feat)).astype(BF)
        for lane in range(2):
            at = z_of_side(2 * g + lane)
            far_out[at] = moved[:, lane * narrow : (lane + 1) * narrow]

            @pl.when(at != z)
            def _():
                far_copy(at).start()

    def run_copy(way, sub, t):
        rows = pl.ds(sub * quarter, quarter)
        return remote(
            run.at[way, t, rows],
            run.at[way, t + 1, rows],
            r_send.at[way, sub, t],
            r_recv.at[way, sub, t],
            on_z(up if way == 0 else down),
        )

    for way in range(2):
        run[way, 0] = jnp.zeros((half, narrow), BF)
    partner_part(0)
    lax.fori_loop(0, nz, side_part, 0)

    def reduce_step(t, carry):
        for way in range(2):
            part_copy(way, t).wait_recv()
            w = wgu[:, half_cols(target_of(way, t) * 2 + c, 0)]
            own = dot(bgu[pl.ds(way * half, half), :], w)
            own_s[way] = own + part_in[way, t].astype(F32)
        for sub in range(2):
            for way in range(2):
                rows = pl.ds(sub * quarter, quarter)

                @pl.when(t > 0)
                def _():
                    run_copy(way, sub, t - 1).wait_recv()

                total = own_s[way, rows] + run[way, t, rows].astype(F32)
                run[way, t, rows] = total.astype(BF)

                @pl.when(t < nz - 1)
                def _():
                    run_copy(way, sub, t).start()

        @pl.when(t < nz - 1)
        def _():
            partner_part(t + 1)

        @pl.when(t < n_groups)
        def _():
            send_group(t)

        for lane in range(2):
            rows = rows_all[0, t, lane].reshape(slots, feat)
            grad_gu[:, cols(t * 2 + lane)] = dot(bgu_t[...], rows)
            rows = rows_all[1, t, lane].reshape(slots, feat)
            grad_d[:, cols(t * 2 + lane)] = dot(hid_t[...], rows)

        @pl.when((t >= 3) & (lax.rem(t, 2) == 1))
        def _():
            take_group(lax.div(t - 3, 2))

        return carry

    lax.fori_loop(0, nz, reduce_step, 0)

    results = [
        pltpu.make_async_copy(grad_gu.at[pl.ds(0, hid)], gg_hbm, o_sem.at[0]),
        pltpu.make_async_copy(grad_gu.at[pl.ds(hid, hid)], gu_hbm, o_sem.at[1]),
        pltpu.make_async_copy(grad_d, gd_hbm, o_sem.at[2]),
    ]

    def back_src(s):
        way, row = lax.div(s, ns // 2), lax.rem(s, ns // 2)
        return run.at[way, nz - 1, pl.ds(pl.multiple_of(row * cap, cap), cap)]

    def back_copy(index, dev, s_to):
        return remote(back_src(s_to), back.at[me], b_send.at[index], b_recv.at[me], dev)

    for index, (dy, dx) in enumerate(shifts):
        dev, s_to = at_plane(dy, dx)
        back_copy(index, dev, s_to).start()
    back[me] = back_src(me)[...]
    for result in results:
        result.start()
    for g in range(max(0, (nz - 2) // 2), n_groups):
        take_group(g)
    for dy, dx in shifts:
        _, s_from = at_plane(dy, dx)
        remote(
            back_src(s_from), back.at[s_from], b_send.at[0], b_recv.at[s_from], partner
        ).wait_recv()
    moe = dot(pick_t[...], back[...].reshape(slots, narrow))
    gm_out[:, :narrow] = (cot[:, :narrow].astype(F32) + moe).astype(BF)
    moe = far_out[z].astype(F32)
    for step in range(1, nz):
        z_from = lax.rem(z + step, nz)
        part = far_in.at[z_from]
        remote(part, part, y_send.at[z_from], y_recv.at[z_from], partner).wait_recv()
        moe = moe + far_in[z_from].astype(F32)
    gm_out[:, narrow:] = (cot[:, narrow:].astype(F32) + moe).astype(BF)
    grad_mixed = gm_out[...]
    full[z, c] = grad_mixed

    def full_part(way, h, k, lane):
        return full.at[along(way, k), lane, pl.ds(h * halves, halves)]

    def full_copy(way, h, k):
        part = full_part(way, h, k, c)
        return remote(
            part, part, f_send.at[way, h, k], f_recv.at[way, h, k], on_z(up if way == 0 else down)
        )

    def full_wait(way, h, k):
        part = full_part(way, h, k, c)
        remote(
            part, part, f_send.at[way, h, k - 1], f_recv.at[way, h, k - 1], partner
        ).wait_recv()

    def full_share(way, h, k, lane):
        part = full_part(way, h, k, lane)
        return remote(part, part, e_send.at[way, h, k], e_recv.at[way, h, k], partner)

    bm_acc[...] = jnp.zeros_like(bm_acc)

    def mixer_products(at):
        for lane in range(2):
            f = full[at, lane]
            bm_acc[...] += dot_nt(op[:, cols(at * 2 + lane)], f)
            proj_out[at * 2 + lane] = dot(act_s[...], f).astype(BF)

    shared = []
    for h in range(2):
        for way in range(2):
            if hops[(way, h)] > 0:
                full_copy(way, h, 0).start()
    for h in range(2):
        full_share(0, h, 0, c).start()
        shared.append((0, h, 0))
    def proj_copy(index, dev, s_to):
        return remote(proj_out.at[s_to], proj_in.at[me], j_send.at[index], j_recv.at[me], dev)

    def proj_send(nearest, furthest):
        for index, (dy, dx) in enumerate(shifts):
            dev, s_to = at_plane(dy, dx)
            off = lax.rem(lax.div(s_to, 2) + nz - z, nz)
            far_enough = (off >= nearest) & (nz - off >= nearest)

            @pl.when(far_enough & ((off <= furthest) | (nz - off <= furthest)))
            def _():
                proj_copy(index, dev, s_to).start()

    pending = [(0, [(0, 0, 0), (0, 1, 0)])]
    for k in range(1, nz // 2 + 1):
        news = {}
        for h in range(2):
            for way in range(2):
                if k > hops[(way, h)]:
                    continue
                full_wait(way, h, k)
                if k < hops[(way, h)]:
                    full_copy(way, h, k).start()
                full_share(way, h, k, c).start()
                shared.append((way, h, k))
                news.setdefault(k if (way == 0 or 2 * k == nz) else -k, []).append((way, h, k))
        for pos, waits in pending:
            for args in waits:
                full_share(*args, other).wait_recv()
            mixer_products(lax.rem(z + nz - pos, nz))
        pending = list(news.items())
        if k > 1:
            proj_send(0 if k == 2 else k - 1, k - 1)
    for pos, waits in pending:
        for args in waits:
            full_share(*args, other).wait_recv()
        mixer_products(lax.rem(z + nz - pos, nz))

    proj_send(nz // 2 if nz > 2 else 0, nz)
    back_mixer = bm_acc[...]
    back_conv = back_mixer * c_outer[...].astype(F32)
    tail_out[...] = back_conv[:, :128]

    def tail_copy(dev):
        return remote(tail_out, tail_in, t_send.at[0], t_recv.at[0], dev)

    tail_copy(on_sp(previous)).start()

    gouter[...] = (back_mixer * conv_s[...]).astype(BF)
    tail_copy(on_sp(following)).wait_recv()
    tail = jnp.where(me == ns - 1, 0.0, tail_in[...])
    ext = jnp.concatenate([back_conv, tail], axis=1)
    width = ext.shape[1]
    back_prod = tap[n_taps - 1] * back_conv
    for j in range(n_taps - 1):
        back_prod = (
            back_prod + tap[j] * pltpu.roll(ext, width - (n_taps - 1 - j), 1)[:, :toks]
        )
    ginner[...] = (back_prod * c_input[...].astype(F32)).astype(BF)
    ginput[...] = (back_prod * c_inner[...].astype(F32)).astype(BF)

    proj_total = proj_out[me].astype(F32)
    for dy, dx in shifts:
        _, s_from = at_plane(dy, dx)
        remote(
            proj_out.at[s_from], proj_in.at[s_from], j_send.at[0], j_recv.at[s_from], partner
        ).wait_recv()
        proj_total = proj_total + proj_in[s_from].astype(F32)
    gproj[...] = proj_total

    for result in results:
        result.wait()
    for index, (dy, dx) in enumerate(shifts):
        dev, s_to = at_plane(dy, dx)
        route_copy(index, dev, s_to).wait_send()
        back_copy(index, dev, s_to).wait_send()
        proj_copy(index, dev, s_to).wait_send()
    for arr in range(2):
        rim_copy(arr, on_sp(following)).wait_send()
    tail_copy(on_sp(previous)).wait_send()

    def ring_sent(t, carry):
        for arr in range(2):
            for sub in range(SUBS):
                ring_copy(arr, sub, t).wait_send()
            for sub in range(2):
                run_copy(arr, sub, t).wait_send()
        return carry

    lax.fori_loop(0, nz - 1, ring_sent, 0)

    def shares_sent(t, carry):
        for way in range(2):
            share(way, t, c).wait_send()
            part_copy(way, t).wait_send()
        cot_share(t, c).wait_send()
        side_copy(t).wait_send()
        for index, (dy, dx) in enumerate(shifts):
            dev, s_to = at_plane(dy, dx)
            cot_copy(t, index, dev, s_to).wait_send()
        return carry

    lax.fori_loop(0, nz, shares_sent, 0)

    def groups_sent(g, carry):
        for index, (dy, dx) in enumerate(shifts):
            dev, s_to = at_plane(dy, dx)
            group_copy(g, index, dev, s_to).wait_send()
        return carry

    lax.fori_loop(0, n_groups, groups_sent, 0)
    for step in range(1, nz):
        far_copy(lax.rem(z + step, nz)).wait_send()
    for (way, h), n in hops.items():
        for k in range(n):
            full_copy(way, h, k).wait_send()
            raw_copy(way, h, k).wait_send()
    for args in shared:
        full_share(*args, c).wait_send()


def finish(*refs):
    from_hbm, from_vmem = refs[0:3], refs[3:8]
    to_hbm, to_vmem = refs[8:11], refs[11:16]
    held, in_sem, out_sem = refs[16:19]
    rows = from_hbm[0].shape[0] // PIECES

    def copy_in(a, p):
        part = pl.ds(p * rows, rows)
        return pltpu.make_async_copy(from_hbm[a].at[part], held.at[a, part], in_sem.at[a, p])

    def copy_out(a, p):
        part = pl.ds(p * rows, rows)
        return pltpu.make_async_copy(held.at[a, part], to_hbm[a].at[part], out_sem.at[a, p])

    pieces = [(a, p) for a in range(3) for p in range(PIECES)]
    for a, p in pieces:
        copy_in(a, p).start()
    for src, dst in zip(from_vmem, to_vmem):
        dst[...] = src[...]
    for a, p in pieces:
        copy_in(a, p).wait()
        copy_out(a, p).start()
    for a, p in pieces:
        copy_out(a, p).wait()


def shards(
    dims,
    conv_outer,
    conv_inner,
    conv_input,
    conv_taps,
    out_proj,
    mixed_state,
    route_ids,
    route_weights,
    w_gate,
    w_up,
    w_down,
    cotangent,
):
    ny, nx, nz = dims
    ns = ny * nx
    toks, feat = mixed_state.shape
    hid, d_all = out_proj.shape[0], out_proj.shape[1]
    chans = conv_outer.shape[0]
    hid = w_gate.shape[1]
    cap = 4 * toks // ns
    slots = ns * cap
    vmem = pl.BlockSpec(memory_space=pltpu.VMEM)
    hbm = pl.BlockSpec(memory_space=pl.ANY)
    dma = pltpu.SemaphoreType.DMA
    scratch = [
        pltpu.VMEM((2, nz, 2, ns, cap, feat), BF),
        pltpu.VMEM((2 * hid, d_all), BF),
        pltpu.VMEM((hid, d_all), BF),
        pltpu.VMEM((chans, d_all), BF),
        pltpu.VMEM((ns, cap, feat), BF),
        pltpu.VMEM((nz, toks, feat), BF),
        pltpu.VMEM((nz, ns, cap, feat), BF),
        pltpu.VMEM((slots, 2 * hid), F32),
        pltpu.VMEM((slots, hid), F32),
        pltpu.VMEM((slots, toks), BF),
        pltpu.VMEM((toks, slots), BF),
        pltpu.VMEM((slots, 2 * hid), BF),
        pltpu.VMEM((2 * hid, slots), BF),
        pltpu.VMEM((hid, slots), BF),
        pltpu.VMEM((2, nz, slots // 2, feat // 2), BF),
        pltpu.VMEM((2, nz, slots // 2, feat // 2), BF),
        pltpu.VMEM((2, nz, slots // 2, feat // 2), BF),
        pltpu.VMEM((2, slots // 2, feat // 2), F32),
        pltpu.VMEM((ns, cap, feat // 2), BF),
        pltpu.VMEM((nz, slots, feat // 2), BF),
        pltpu.VMEM((nz, slots, feat // 2), BF),
        pltpu.VMEM((nz // 2, ns, cap, feat), BF),
        pltpu.VMEM((nz // 2, ns, cap, feat), BF),
        pltpu.VMEM((nz, toks, feat // 2), BF),
        pltpu.VMEM((nz, toks, feat // 2), BF),
        pltpu.VMEM((2 * hid, d_all), F32),
        pltpu.VMEM((hid, d_all), F32),
        pltpu.VMEM((nz, 2, toks, feat), BF),
        pltpu.VMEM((nz * 2, chans, feat), BF),
        pltpu.VMEM((ns, chans, feat), BF),
        pltpu.VMEM((2, chans, 128), BF),
        pltpu.VMEM((chans, 128), F32),
        pltpu.VMEM((chans, 128), F32),
        pltpu.VMEM((chans, toks), F32),
        pltpu.VMEM((chans, toks), BF),
        pltpu.VMEM((chans, toks), F32),
        dma((4,)),
        dma((3,)),
        dma((ns,)),
        dma((ns,)),
        dma((2, SUBS, nz)),
        dma((2, SUBS, nz)),
        dma((2, nz)),
        dma((2, nz)),
        dma((2, 2, nz)),
        dma((2, 2, nz)),
        dma((nz, ns)),
        dma((nz, ns)),
        dma((nz,)),
        dma((nz,)),
        dma((2, nz)),
        dma((2, nz)),
        dma((2, 2, nz)),
        dma((2, 2, nz)),
        dma((ns,)),
        dma((ns,)),
        dma((2, 2, nz)),
        dma((2, 2, nz)),
        dma((2, 2, nz)),
        dma((2, 2, nz)),
        dma((ns,)),
        dma((ns,)),
        dma((2,)),
        dma((2,)),
        dma((1,)),
        dma((1,)),
        dma((nz,)),
        dma((nz,)),
        dma((nz // 2, ns)),
        dma((nz // 2, ns)),
        dma((nz,)),
        dma((nz,)),
    ]
    grad = jax.ShapeDtypeStruct((hid, d_all), F32)
    conv = jax.ShapeDtypeStruct((chans, toks), BF)
    outs = pl.pallas_call(
        functools.partial(kernel, dims),
        out_shape=(
            grad,
            grad,
            grad,
            jax.ShapeDtypeStruct((toks, feat), BF),
            jax.ShapeDtypeStruct((chans, feat), F32),
            conv,
            conv,
            conv,
        ),
        in_specs=[vmem] * 8 + [hbm] * 4,
        out_specs=(hbm,) * 3 + (vmem,) * 5,
        scratch_shapes=scratch,
        compiler_params=pltpu.CompilerParams(
            collective_id=0, has_side_effects=True, vmem_limit_bytes=66000000
        ),
    )(
        route_ids.T,
        route_weights.T,
        mixed_state,
        cotangent,
        conv_outer,
        conv_inner,
        conv_input,
        conv_taps,
        w_gate[0],
        w_up[0],
        w_down[0],
        out_proj,
    )
    outs = pl.pallas_call(
        finish,
        out_shape=tuple(jax.ShapeDtypeStruct(o.shape, o.dtype) for o in outs),
        in_specs=[hbm] * 3 + [vmem] * 5,
        out_specs=(hbm,) * 3 + (vmem,) * 5,
        scratch_shapes=[pltpu.VMEM((3, hid, d_all), F32), dma((3, PIECES)), dma((3, PIECES))],
        compiler_params=pltpu.CompilerParams(vmem_limit_bytes=62000000),
    )(*outs)
    return (outs[0][None], outs[1][None], outs[2][None], *outs[3:])


def solution(mesh):
    dims = (4, 4, 8)
    return on_torus(Mesh(mesh.devices.reshape(*dims, 2), ("y", "x", "z", "c")), dims)


def on_torus(torus, dims):
    sp, tp = ("y", "x"), ("z", "c")
    return jax.shard_map(
        functools.partial(shards, dims),
        mesh=torus,
        in_specs=(
            P(tp, sp),
            P(tp, sp),
            P(tp, sp),
            P(None, tp),
            P(tp, None),
            P(sp, tp),
            P(sp, None),
            P(sp, None),
            P(sp, tp, None),
            P(sp, tp, None),
            P(sp, tp, None),
            P(sp, tp),
        ),
        out_specs=(
            P(sp, tp, None),
            P(sp, tp, None),
            P(sp, tp, None),
            P(sp, tp),
            P(tp, sp),
            P(tp, sp),
            P(tp, sp),
            P(tp, sp),
        ),
        check_vma=False,
    )
```

```python
import functools

import jax
import jax.numpy as jnp
from jax import lax
from jax.experimental import pallas as pl
from jax.experimental.pallas import tpu as pltpu
from jax.sharding import Mesh
from jax.sharding import PartitionSpec as P

BF = jnp.bfloat16
F32 = jnp.float32
MESH_ID = pl.DeviceIdType.MESH
SUBS = 2
PIECES = 4
EARLY = 3
PARTS = 4


def dot(a, b):
    return lax.dot_general(a, b, (((1,), (0,)), ((), ())), preferred_element_type=F32)


def dot_nt(a, b):
    return lax.dot_general(a, b, (((1,), (1,)), ((), ())), preferred_element_type=F32)


def kernel(
    dims,
    ids,
    wts,
    state,
    cot,
    c_outer,
    c_inner,
    c_input,
    taps,
    wg_hbm,
    wu_hbm,
    wd_hbm,
    op_hbm,
    gg_hbm,
    gu_hbm,
    gd_hbm,
    gm_out,
    gproj,
    gouter,
    ginner,
    ginput,
    rows_all,
    wgu,
    wd,
    op,
    sent,
    raw,
    routed,
    acc_gu,
    acc_d,
    pick,
    pick_t,
    bgu,
    bgu_t,
    hid_t,
    part_out,
    part_in,
    run,
    own_s,
    back,
    side_out,
    side_in,
    group_out,
    group_in,
    far_out,
    far_in,
    grad_gu,
    grad_d,
    full,
    proj_out,
    proj_in,
    rim_in,
    tail_out,
    tail_in,
    conv_s,
    act_s,
    bm_acc,
    w_sem,
    o_sem,
    a_send,
    a_recv,
    g_send,
    g_recv,
    d_send,
    d_recv,
    c_send,
    c_recv,
    q_send,
    q_recv,
    s_send,
    s_recv,
    p_send,
    p_recv,
    r_send,
    r_recv,
    b_send,
    b_recv,
    f_send,
    f_recv,
    e_send,
    e_recv,
    j_send,
    j_recv,
    h_send,
    h_recv,
    t_send,
    t_recv,
    u_send,
    u_recv,
    v_send,
    v_recv,
    y_send,
    y_recv,
):
    ny, nx, nz = dims
    ns = ny * nx
    hid, d_all = wg_hbm.shape
    toks, feat = state.shape
    cap = sent.shape[1]
    slots = ns * cap
    y, x = lax.axis_index("y"), lax.axis_index("x")
    z, c = lax.axis_index("z"), lax.axis_index("c")
    me = y * nx + x
    other = 1 - c
    up, down = lax.rem(z + 1, nz), lax.rem(z + nz - 1, nz)
    shifts = [(dy, dx) for dy in range(ny) for dx in range(nx) if (dy, dx) != (0, 0)]
    following, previous = lax.rem(me + 1, ns), lax.rem(me + ns - 1, ns)

    def at_plane(dy, dx):
        py, px = lax.rem(y + dy, ny), lax.rem(x + dx, nx)
        return {"y": py, "x": px, "z": z, "c": c}, py * nx + px

    def on_sp(s):
        return {"y": lax.div(s, nx), "x": lax.rem(s, nx), "z": z, "c": c}

    def on_z(pos):
        return {"y": y, "x": x, "z": pos, "c": c}

    partner = {"y": y, "x": x, "z": z, "c": other}

    def remote(src, dst, send, recv, device):
        return pltpu.make_async_remote_copy(
            src_ref=src,
            dst_ref=dst,
            send_sem=send,
            recv_sem=recv,
            device_id=device,
            device_id_type=MESH_ID,
        )

    def half_cols(index, off):
        return pl.ds(pl.multiple_of(index * feat + off, feat // 2), feat // 2)

    def cols(index):
        return pl.ds(pl.multiple_of(index * feat, feat), feat)

    loads = [
        pltpu.make_async_copy(wg_hbm, wgu.at[pl.ds(0, hid)], w_sem.at[0]),
        pltpu.make_async_copy(wu_hbm, wgu.at[pl.ds(hid, hid)], w_sem.at[1]),
        pltpu.make_async_copy(wd_hbm, wd, w_sem.at[2]),
        pltpu.make_async_copy(op_hbm, op, w_sem.at[3]),
    ]
    for load in loads:
        load.start()

    barrier = pltpu.get_barrier_semaphore()
    peers = [at_plane(dy, dx)[0] for dy, dx in shifts] + [partner]
    peers += [on_z(lax.rem(z + step, nz)) for step in range(1, nz)]
    for peer in peers:
        pl.semaphore_signal(barrier, inc=1, device_id=peer, device_id_type=MESH_ID)

    pl.semaphore_wait(barrier, len(peers))

    halves = toks // PARTS
    hops = {}
    for h in range(PARTS):
        late = 2 * h // PARTS
        hops[(0, h)], hops[(1, h)] = nz // 2 - late, nz // 2 - 1 + late

    def along(way, k):
        return lax.rem(z + nz - k, nz) if way == 0 else lax.rem(z + k, nz)

    def raw_copy(way, h, k):
        rows = pl.ds(h * halves, halves)
        src = cot.at[rows] if k == 0 else raw.at[along(way, k), rows]
        return remote(
            src,
            raw.at[along(way, k), rows],
            c_send.at[way, h, k],
            c_recv.at[way, h, k],
            on_z(up if way == 0 else down),
        )

    def raw_wait(way, h, k):
        part = raw.at[along(way, k), pl.ds(h * halves, halves)]
        remote(
            part, part, c_send.at[way, h, k - 1], c_recv.at[way, h, k - 1], partner
        ).wait_recv()

    for h in range(PARTS):
        for way in range(2):
            if hops[(way, h)] > 0:
                raw_copy(way, h, 0).start()

    expert = lax.broadcasted_iota(jnp.int32, (ns, toks), 0)
    first, second = ids[0:1, :] == expert, ids[1:2, :] == expert
    named = jnp.where(first, 1.0, 0.0) + jnp.where(second, 1.0, 0.0)
    weight = jnp.where(first, wts[0:1, :], 0.0) + jnp.where(second, wts[1:2, :], 0.0)
    earlier = jnp.where(
        lax.broadcasted_iota(jnp.int32, (toks, toks), 0)
        < lax.broadcasted_iota(jnp.int32, (toks, toks), 1),
        1.0,
        0.0,
    ).astype(BF)
    count = jnp.where(named > 0.0, dot(named.astype(BF), earlier), -1.0)
    place = lax.broadcasted_iota(jnp.int32, (cap, toks), 0).astype(F32)
    scales = []
    for e in range(ns):
        hit = jnp.where(count[e : e + 1, :] == place, 1.0, 0.0)
        pick[pl.ds(e * cap, cap), :] = hit.astype(BF)
        scales.append(jnp.sum(hit * weight[e : e + 1, :], axis=1, keepdims=True))
    scale = jnp.concatenate(scales, axis=0)
    sent[...] = dot(pick[...], state[...]).astype(BF).reshape(ns, cap, feat)

    def route_copy(index, dev, s_to):
        return remote(
            sent.at[s_to], rows_all.at[0, z, c, me], a_send.at[index], a_recv.at[me], dev
        )

    def route_wait(s_from):
        part = rows_all.at[0, z, c, s_from]
        remote(part, part, a_send.at[0], a_recv.at[s_from], partner).wait_recv()

    for index, (dy, dx) in enumerate(shifts):
        dev, s_to = at_plane(dy, dx)
        route_copy(index, dev, s_to).start()
    rows_all[0, z, c, me] = sent[me]

    def rim_copy(arr, dev):
        src = (c_inner, c_input)[arr]
        lanes = src.shape[1]
        return remote(
            src.at[:, pl.ds(lanes - 128, 128)], rim_in.at[arr], h_send.at[arr], h_recv.at[arr], dev
        )

    for arr in range(2):
        rim_copy(arr, on_sp(following)).start()

    def z_of(i):
        step = lax.div(i + 1, 2)
        return lax.rem(z + nz + step * (1 - 2 * lax.rem(i, 2)), nz)

    def cot_copy(i, index, dev, s_to):
        return remote(
            routed.at[i, s_to],
            rows_all.at[1, z_of(i), c, me],
            q_send.at[i, index],
            q_recv.at[i, me],
            dev,
        )

    def cot_wait(i, s_from):
        part = rows_all.at[1, z_of(i), c, s_from]
        remote(part, part, q_send.at[i, 0], q_recv.at[i, s_from], partner).wait_recv()

    def cot_route(i, rows):
        picked = dot(pick[...], rows) * scale
        routed[i] = picked.astype(BF).reshape(ns, cap, feat)
        for index, (dy, dx) in enumerate(shifts):
            dev, s_to = at_plane(dy, dx)
            cot_copy(i, index, dev, s_to).start()
        rows_all[1, z_of(i), c, me] = routed[i, me]

    acc_gu[...] = jnp.zeros_like(acc_gu)
    acc_d[...] = jnp.zeros_like(acc_d)
    half = slots // 2
    ring_s = ns // 2
    per_sub = ring_s // SUBS

    def ring_copy(way, sub, t):
        part = rows_all.at[0, along(way, t), c, pl.ds(way * ring_s + sub * per_sub, per_sub)]
        return remote(
            part,
            part,
            g_send.at[way, sub, t],
            g_recv.at[way, sub, t],
            on_z(up if way == 0 else down),
        )

    def ring_wait(way, sub, t):
        part = rows_all.at[0, along(way, t), c, pl.ds(way * ring_s + sub * per_sub, per_sub)]
        remote(
            part, part, g_send.at[way, sub, t - 1], g_recv.at[way, sub, t - 1], partner
        ).wait_recv()

    def share(way, t, lane):
        part = rows_all.at[0, along(way, t), lane, pl.ds(way * ring_s, ring_s)]
        return remote(part, part, d_send.at[way, t], d_recv.at[way, t], partner)

    def cot_share(i, lane):
        part = rows_all.at[1, z_of(i), lane]
        return remote(part, part, s_send.at[i], s_recv.at[i], partner)

    def state_products(t):
        for way in range(2):
            share(way, t, other).wait_recv()
        for way in range(2):
            at = along(way, t)
            for lane in range(2):
                rows = rows_all[0, at, lane, way * ring_s : (way + 1) * ring_s]
                acc_gu[way * half : (way + 1) * half, :] += dot_nt(
                    rows.reshape(half, feat), wgu[:, cols(at * 2 + lane)]
                )

    def cot_products(i):
        cot_share(i, other).wait_recv()
        for lane in range(2):
            rows = rows_all[1, z_of(i), lane].reshape(slots, feat)
            acc_d[...] += dot_nt(rows, wd[:, cols(z_of(i) * 2 + lane)])

    def cot_arrived(i):
        for dy, dx in shifts:
            cot_wait(i, at_plane(dy, dx)[1])
        cot_share(i, c).start()

    for sub in range(SUBS):
        for way in range(2):
            first_s = way * ring_s + sub * per_sub
            for s_from in range(first_s, first_s + per_sub):

                @pl.when(s_from != me)
                def _():
                    route_wait(s_from)

            ring_copy(way, sub, 0).start()
    for way in range(2):
        share(way, 0, c).start()
    cot_route(0, cot[...])
    for load in loads:
        load.wait()

    def ring_step(t):
        for sub in range(SUBS):
            for way in range(2):
                ring_wait(way, sub, t)

                @pl.when(t < nz - 1)
                def _():
                    ring_copy(way, sub, t).start()

        for way in range(2):
            share(way, t, c).start()

    for k in range(1, nz // 2 + 1):
        for h in range(PARTS):
            for way in range(2):
                if k <= hops[(way, h)]:
                    raw_wait(way, h, k)
                    if k < hops[(way, h)]:
                        raw_copy(way, h, k).start()
        cot_route(2 * k - 1, raw[along(0, k)])
        if 2 * k < nz:
            cot_route(2 * k, raw[along(1, k)])
        if k < min(nz, EARLY + 1):
            ring_step(k)

    for arr in range(2):
        rim_copy(arr, on_sp(previous)).wait_recv()
    inner, inp = c_inner[...].astype(F32), c_input[...].astype(F32)
    rim_prod = rim_in[0].astype(F32) * rim_in[1].astype(F32)
    rim_prod = jnp.where(me == 0, 0.0, rim_prod)
    ext = jnp.concatenate([rim_prod, inner * inp], axis=1)
    n_taps, chans = taps.shape
    diagonal = lax.broadcasted_iota(jnp.int32, (chans, chans), 0) == lax.broadcasted_iota(
        jnp.int32, (chans, chans), 1
    )
    tap = [
        jnp.sum(jnp.where(diagonal, taps[j : j + 1, :], 0.0), axis=1, keepdims=True)
        for j in range(n_taps)
    ]
    conv_out = tap[n_taps - 1] * (inner * inp)
    for j in range(n_taps - 1):
        conv_out = conv_out + tap[j] * pltpu.roll(ext, n_taps - 1 - j, 1)[:, 128:]
    conv_s[...] = conv_out
    act_s[...] = (c_outer[...].astype(F32) * conv_out).astype(BF)
    pick_t[...] = pick[...].T

    def gather_step(t, carry):
        @pl.when(t > EARLY)
        def _():
            ring_step(t)

        cot_arrived(t - 1)
        state_products(t - 1)

        @pl.when(t > 1)
        def _():
            cot_products(t - 2)

        return carry

    lax.fori_loop(1, nz, gather_step, 0)
    cot_arrived(nz - 1)
    state_products(nz - 1)
    if nz > 1:
        cot_products(nz - 2)
    cot_products(nz - 1)

    gate_pre, up_pre = acc_gu[:, :hid], acc_gu[:, hid:]
    back_hidden = acc_d[...]
    sig = jax.nn.sigmoid(gate_pre)
    silu = gate_pre * sig
    hid_t[...] = (silu * up_pre).astype(BF).T
    back_gate = (back_hidden * up_pre * sig * (1.0 + gate_pre * (1.0 - sig))).astype(BF)
    back_up = (back_hidden * silu).astype(BF)
    bgu[:, :hid] = back_gate
    bgu[:, hid:] = back_up
    bgu_t[:hid, :] = back_gate.T
    bgu_t[hid:, :] = back_up.T

    quarter = half // 2

    def target_of(way, t):
        return lax.rem(z + 2 * nz - 1 - t, nz) if way == 0 else lax.rem(z + 1 + t, nz)

    def part_copy(way, t):
        return remote(
            part_out.at[way, t], part_in.at[way, t], p_send.at[way, t], p_recv.at[way, t], partner
        )

    def partner_part(t):
        for way in range(2):
            w = wgu[:, half_cols(target_of(way, t) * 2 + other, 0)]
            part_out[way, t] = dot(bgu[pl.ds(way * half, half), :], w).astype(BF)
            part_copy(way, t).start()

    n_groups = nz // 2
    narrow = feat // 2

    def z_of_side(j):
        return lax.rem(lax.div(z, 2) + 1 + lax.div(j, 2), n_groups) * 2 + lax.rem(j, 2)

    def side_copy(j):
        return remote(side_out.at[j], side_in.at[j], u_send.at[j], u_recv.at[j], partner)

    def side_part(j):
        w = wgu[:, half_cols(z_of_side(j) * 2 + other, narrow)]
        side_out[j] = dot(bgu[...], w).astype(BF)
        side_copy(j).start()

    def group_copy(g, index, dev, s_to):
        return remote(
            group_out.at[g, s_to], group_in.at[g, me], v_send.at[g, index], v_recv.at[g, me], dev
        )

    def send_group(g):
        for lane in range(2):
            j = 2 * g + lane
            side_copy(j).wait_recv()
            w = wgu[:, half_cols(z_of_side(j) * 2 + c, narrow)]
            total = dot(bgu[...], w) + side_in[j].astype(F32)
            group_out[g, :, :, lane * narrow : (lane + 1) * narrow] = total.astype(BF).reshape(
                ns, cap, narrow
            )
        for index, (dy, dx) in enumerate(shifts):
            dev, s_to = at_plane(dy, dx)
            group_copy(g, index, dev, s_to).start()
        group_in[g, me] = group_out[g, me]

    def far_copy(at):
        return remote(far_out.at[at], far_in.at[z], y_send.at[at], y_recv.at[z], on_z(at))

    def take_group(g):
        for dy, dx in shifts:
            s_from = at_plane(dy, dx)[1]
            part = group_in.at[g, s_from]
            remote(part, part, v_send.at[g, 0], v_recv.at[g, s_from], partner).wait_recv()
        moved = dot(pick_t[...], group_in[g].reshape(slots, feat)).astype(BF)
        for lane in range(2):
            at = z_of_side(2 * g + lane)
            far_out[at] = moved[:, lane * narrow : (lane + 1) * narrow]

            @pl.when(at != z)
            def _():
                far_copy(at).start()

    def run_copy(way, sub, t):
        rows = pl.ds(sub * quarter, quarter)
        return remote(
            run.at[way, t, rows],
            run.at[way, t + 1, rows],
            r_send.at[way, sub, t],
            r_recv.at[way, sub, t],
            on_z(up if way == 0 else down),
        )

    for way in range(2):
        run[way, 0] = jnp.zeros((half, narrow), BF)
    partner_part(0)
    side_part(0)
    side_part(1)

    def reduce_step(t, carry):
        for way in range(2):
            part_copy(way, t).wait_recv()
            w = wgu[:, half_cols(target_of(way, t) * 2 + c, 0)]
            own = dot(bgu[pl.ds(way * half, half), :], w)
            own_s[way] = own + part_in[way, t].astype(F32)
        for sub in range(2):
            for way in range(2):
                rows = pl.ds(sub * quarter, quarter)

                @pl.when(t > 0)
                def _():
                    run_copy(way, sub, t - 1).wait_recv()

                total = own_s[way, rows] + run[way, t, rows].astype(F32)
                run[way, t, rows] = total.astype(BF)

                @pl.when(t < nz - 1)
                def _():
                    run_copy(way, sub, t).start()

        @pl.when(t < nz - 1)
        def _():
            partner_part(t + 1)

        @pl.when(t < n_groups)
        def _():
            send_group(t)

        @pl.when(t < n_groups - 1)
        def _():
            side_part(2 * t + 2)
            side_part(2 * t + 3)

        for lane in range(2):
            rows = rows_all[0, t, lane].reshape(slots, feat)
            grad_gu[:, cols(t * 2 + lane)] = dot(bgu_t[...], rows)
            rows = rows_all[1, t, lane].reshape(slots, feat)
            grad_d[:, cols(t * 2 + lane)] = dot(hid_t[...], rows)

        @pl.when((t >= 2) & (lax.rem(t, 2) == 0))
        def _():
            take_group(lax.div(t - 2, 2))

        return carry

    lax.fori_loop(0, nz, reduce_step, 0)

    results = [
        pltpu.make_async_copy(grad_gu.at[pl.ds(0, hid)], gg_hbm, o_sem.at[0]),
        pltpu.make_async_copy(grad_gu.at[pl.ds(hid, hid)], gu_hbm, o_sem.at[1]),
        pltpu.make_async_copy(grad_d, gd_hbm, o_sem.at[2]),
    ]

    def back_src(s):
        way, row = lax.div(s, ns // 2), lax.rem(s, ns // 2)
        return run.at[way, nz - 1, pl.ds(pl.multiple_of(row * cap, cap), cap)]

    def back_copy(index, dev, s_to):
        return remote(back_src(s_to), back.at[me], b_send.at[index], b_recv.at[me], dev)

    for index, (dy, dx) in enumerate(shifts):
        dev, s_to = at_plane(dy, dx)
        back_copy(index, dev, s_to).start()
    back[me] = back_src(me)[...]
    for result in results:
        result.start()
    for g in range(max(0, (nz - 2) // 2), n_groups):
        take_group(g)
    for dy, dx in shifts:
        _, s_from = at_plane(dy, dx)
        remote(
            back_src(s_from), back.at[s_from], b_send.at[0], b_recv.at[s_from], partner
        ).wait_recv()
    moe = dot(pick_t[...], back[...].reshape(slots, narrow))
    gm_out[:, :narrow] = (cot[:, :narrow].astype(F32) + moe).astype(BF)
    moe = far_out[z].astype(F32)
    for step in range(1, nz):
        z_from = lax.rem(z + step, nz)
        part = far_in.at[z_from]
        remote(part, part, y_send.at[z_from], y_recv.at[z_from], partner).wait_recv()
        moe = moe + far_in[z_from].astype(F32)
    gm_out[:, narrow:] = (cot[:, narrow:].astype(F32) + moe).astype(BF)
    grad_mixed = gm_out[...]
    full[z, c] = grad_mixed

    def full_part(way, h, k, lane):
        return full.at[along(way, k), lane, pl.ds(h * halves, halves)]

    def full_copy(way, h, k):
        part = full_part(way, h, k, c)
        return remote(
            part, part, f_send.at[way, h, k], f_recv.at[way, h, k], on_z(up if way == 0 else down)
        )

    def full_wait(way, h, k):
        part = full_part(way, h, k, c)
        remote(
            part, part, f_send.at[way, h, k - 1], f_recv.at[way, h, k - 1], partner
        ).wait_recv()

    def full_share(way, h, k, lane):
        part = full_part(way, h, k, lane)
        return remote(part, part, e_send.at[way, h, k], e_recv.at[way, h, k], partner)

    bm_acc[...] = jnp.zeros_like(bm_acc)

    def mixer_products(at):
        for lane in range(2):
            f = full[at, lane]
            bm_acc[...] += dot_nt(op[:, cols(at * 2 + lane)], f)
            proj_out[at * 2 + lane] = dot(act_s[...], f).astype(BF)

    shared = []
    for h in range(PARTS):
        for way in range(2):
            if hops[(way, h)] > 0:
                full_copy(way, h, 0).start()
    for h in range(PARTS):
        full_share(0, h, 0, c).start()
        shared.append((0, h, 0))
    def proj_copy(index, dev, s_to):
        return remote(proj_out.at[s_to], proj_in.at[me], j_send.at[index], j_recv.at[me], dev)

    def proj_send(nearest, furthest):
        for index, (dy, dx) in enumerate(shifts):
            dev, s_to = at_plane(dy, dx)
            off = lax.rem(lax.div(s_to, 2) + nz - z, nz)
            far_enough = (off >= nearest) & (nz - off >= nearest)

            @pl.when(far_enough & ((off <= furthest) | (nz - off <= furthest)))
            def _():
                proj_copy(index, dev, s_to).start()

    pending = [(0, [(0, h, 0) for h in range(PARTS)])]
    for k in range(1, nz // 2 + 1):
        news = {}
        for h in range(PARTS):
            for way in range(2):
                if k > hops[(way, h)]:
                    continue
                full_wait(way, h, k)
                if k < hops[(way, h)]:
                    full_copy(way, h, k).start()
                full_share(way, h, k, c).start()
                shared.append((way, h, k))
                news.setdefault(k if (way == 0 or 2 * k == nz) else -k, []).append((way, h, k))
        for pos, waits in pending:
            for args in waits:
                full_share(*args, other).wait_recv()
            mixer_products(lax.rem(z + nz - pos, nz))
        pending = list(news.items())
        if k > 1:
            proj_send(0 if k == 2 else k - 1, k - 1)
    for pos, waits in pending:
        for args in waits:
            full_share(*args, other).wait_recv()
        mixer_products(lax.rem(z + nz - pos, nz))

    back_mixer = bm_acc[...]
    back_conv = back_mixer * c_outer[...].astype(F32)
    tail_out[...] = back_conv[:, :128].T[:8, :]

    def tail_copy(dev):
        return remote(tail_out, tail_in, t_send.at[0], t_recv.at[0], dev)

    tail_copy(on_sp(previous)).start()
    proj_send(nz // 2 if nz > 2 else 0, nz)

    gouter[...] = (back_mixer * conv_s[...]).astype(BF)
    tail_copy(on_sp(following)).wait_recv()
    tail = jnp.concatenate([tail_in[...], jnp.zeros((120, tail_in.shape[1]), F32)], axis=0).T
    tail = jnp.where(me == ns - 1, 0.0, tail)
    ext = jnp.concatenate([back_conv, tail], axis=1)
    width = ext.shape[1]
    back_prod = tap[n_taps - 1] * back_conv
    for j in range(n_taps - 1):
        back_prod = (
            back_prod + tap[j] * pltpu.roll(ext, width - (n_taps - 1 - j), 1)[:, :toks]
        )
    ginner[...] = (back_prod * c_input[...].astype(F32)).astype(BF)
    ginput[...] = (back_prod * c_inner[...].astype(F32)).astype(BF)

    proj_total = proj_out[me].astype(F32)
    for dy, dx in shifts:
        _, s_from = at_plane(dy, dx)
        remote(
            proj_out.at[s_from], proj_in.at[s_from], j_send.at[0], j_recv.at[s_from], partner
        ).wait_recv()
        proj_total = proj_total + proj_in[s_from].astype(F32)
    gproj[...] = proj_total

    for result in results:
        result.wait()
    for index, (dy, dx) in enumerate(shifts):
        dev, s_to = at_plane(dy, dx)
        route_copy(index, dev, s_to).wait_send()
        back_copy(index, dev, s_to).wait_send()
        proj_copy(index, dev, s_to).wait_send()
    for arr in range(2):
        rim_copy(arr, on_sp(following)).wait_send()
    tail_copy(on_sp(previous)).wait_send()

    def ring_sent(t, carry):
        for arr in range(2):
            for sub in range(SUBS):
                ring_copy(arr, sub, t).wait_send()
            for sub in range(2):
                run_copy(arr, sub, t).wait_send()
        return carry

    lax.fori_loop(0, nz - 1, ring_sent, 0)

    def shares_sent(t, carry):
        for way in range(2):
            share(way, t, c).wait_send()
            part_copy(way, t).wait_send()
        cot_share(t, c).wait_send()
        side_copy(t).wait_send()
        for index, (dy, dx) in enumerate(shifts):
            dev, s_to = at_plane(dy, dx)
            cot_copy(t, index, dev, s_to).wait_send()
        return carry

    lax.fori_loop(0, nz, shares_sent, 0)

    def groups_sent(g, carry):
        for index, (dy, dx) in enumerate(shifts):
            dev, s_to = at_plane(dy, dx)
            group_copy(g, index, dev, s_to).wait_send()
        return carry

    lax.fori_loop(0, n_groups, groups_sent, 0)
    for step in range(1, nz):
        far_copy(lax.rem(z + step, nz)).wait_send()
    for (way, h), n in hops.items():
        for k in range(n):
            full_copy(way, h, k).wait_send()
            raw_copy(way, h, k).wait_send()
    for args in shared:
        full_share(*args, c).wait_send()


def finish(*refs):
    from_hbm, from_vmem = refs[0:3], refs[3:8]
    to_hbm, to_vmem = refs[8:11], refs[11:16]
    held, in_sem, out_sem = refs[16:19]
    rows = from_hbm[0].shape[0] // PIECES

    def copy_in(a, p):
        part = pl.ds(p * rows, rows)
        return pltpu.make_async_copy(from_hbm[a].at[part], held.at[a, part], in_sem.at[a, p])

    def copy_out(a, p):
        part = pl.ds(p * rows, rows)
        return pltpu.make_async_copy(held.at[a, part], to_hbm[a].at[part], out_sem.at[a, p])

    pieces = [(a, p) for a in range(3) for p in range(PIECES)]
    for a, p in pieces:
        copy_in(a, p).start()
    for src, dst in zip(from_vmem, to_vmem):
        dst[...] = src[...]
    for a, p in pieces:
        copy_in(a, p).wait()
        copy_out(a, p).start()
    for a, p in pieces:
        copy_out(a, p).wait()


def shards(
    dims,
    conv_outer,
    conv_inner,
    conv_input,
    conv_taps,
    out_proj,
    mixed_state,
    route_ids,
    route_weights,
    w_gate,
    w_up,
    w_down,
    cotangent,
):
    ny, nx, nz = dims
    ns = ny * nx
    toks, feat = mixed_state.shape
    hid, d_all = out_proj.shape[0], out_proj.shape[1]
    chans = conv_outer.shape[0]
    hid = w_gate.shape[1]
    cap = 4 * toks // ns
    slots = ns * cap
    vmem = pl.BlockSpec(memory_space=pltpu.VMEM)
    hbm = pl.BlockSpec(memory_space=pl.ANY)
    dma = pltpu.SemaphoreType.DMA
    scratch = [
        pltpu.VMEM((2, nz, 2, ns, cap, feat), BF),
        pltpu.VMEM((2 * hid, d_all), BF),
        pltpu.VMEM((hid, d_all), BF),
        pltpu.VMEM((chans, d_all), BF),
        pltpu.VMEM((ns, cap, feat), BF),
        pltpu.VMEM((nz, toks, feat), BF),
        pltpu.VMEM((nz, ns, cap, feat), BF),
        pltpu.VMEM((slots, 2 * hid), F32),
        pltpu.VMEM((slots, hid), F32),
        pltpu.VMEM((slots, toks), BF),
        pltpu.VMEM((toks, slots), BF),
        pltpu.VMEM((slots, 2 * hid), BF),
        pltpu.VMEM((2 * hid, slots), BF),
        pltpu.VMEM((hid, slots), BF),
        pltpu.VMEM((2, nz, slots // 2, feat // 2), BF),
        pltpu.VMEM((2, nz, slots // 2, feat // 2), BF),
        pltpu.VMEM((2, nz, slots // 2, feat // 2), BF),
        pltpu.VMEM((2, slots // 2, feat // 2), F32),
        pltpu.VMEM((ns, cap, feat // 2), BF),
        pltpu.VMEM((nz, slots, feat // 2), BF),
        pltpu.VMEM((nz, slots, feat // 2), BF),
        pltpu.VMEM((nz // 2, ns, cap, feat), BF),
        pltpu.VMEM((nz // 2, ns, cap, feat), BF),
        pltpu.VMEM((nz, toks, feat // 2), BF),
        pltpu.VMEM((nz, toks, feat // 2), BF),
        pltpu.VMEM((2 * hid, d_all), F32),
        pltpu.VMEM((hid, d_all), F32),
        pltpu.VMEM((nz, 2, toks, feat), BF),
        pltpu.VMEM((nz * 2, chans, feat), BF),
        pltpu.VMEM((ns, chans, feat), BF),
        pltpu.VMEM((2, chans, 128), BF),
        pltpu.VMEM((8, chans), F32),
        pltpu.VMEM((8, chans), F32),
        pltpu.VMEM((chans, toks), F32),
        pltpu.VMEM((chans, toks), BF),
        pltpu.VMEM((chans, toks), F32),
        dma((4,)),
        dma((3,)),
        dma((ns,)),
        dma((ns,)),
        dma((2, SUBS, nz)),
        dma((2, SUBS, nz)),
        dma((2, nz)),
        dma((2, nz)),
        dma((2, PARTS, nz)),
        dma((2, PARTS, nz)),
        dma((nz, ns)),
        dma((nz, ns)),
        dma((nz,)),
        dma((nz,)),
        dma((2, nz)),
        dma((2, nz)),
        dma((2, 2, nz)),
        dma((2, 2, nz)),
        dma((ns,)),
        dma((ns,)),
        dma((2, PARTS, nz)),
        dma((2, PARTS, nz)),
        dma((2, PARTS, nz)),
        dma((2, PARTS, nz)),
        dma((ns,)),
        dma((ns,)),
        dma((2,)),
        dma((2,)),
        dma((1,)),
        dma((1,)),
        dma((nz,)),
        dma((nz,)),
        dma((nz // 2, ns)),
        dma((nz // 2, ns)),
        dma((nz,)),
        dma((nz,)),
    ]
    grad = jax.ShapeDtypeStruct((hid, d_all), F32)
    conv = jax.ShapeDtypeStruct((chans, toks), BF)
    outs = pl.pallas_call(
        functools.partial(kernel, dims),
        out_shape=(
            grad,
            grad,
            grad,
            jax.ShapeDtypeStruct((toks, feat), BF),
            jax.ShapeDtypeStruct((chans, feat), F32),
            conv,
            conv,
            conv,
        ),
        in_specs=[vmem] * 8 + [hbm] * 4,
        out_specs=(hbm,) * 3 + (vmem,) * 5,
        scratch_shapes=scratch,
        compiler_params=pltpu.CompilerParams(
            collective_id=0, has_side_effects=True, vmem_limit_bytes=66000000
        ),
    )(
        route_ids.T,
        route_weights.T,
        mixed_state,
        cotangent,
        conv_outer,
        conv_inner,
        conv_input,
        conv_taps,
        w_gate[0],
        w_up[0],
        w_down[0],
        out_proj,
    )
    outs = pl.pallas_call(
        finish,
        out_shape=tuple(jax.ShapeDtypeStruct(o.shape, o.dtype) for o in outs),
        in_specs=[hbm] * 3 + [vmem] * 5,
        out_specs=(hbm,) * 3 + (vmem,) * 5,
        scratch_shapes=[pltpu.VMEM((3, hid, d_all), F32), dma((3, PIECES)), dma((3, PIECES))],
        compiler_params=pltpu.CompilerParams(vmem_limit_bytes=62000000),
    )(*outs)
    return (outs[0][None], outs[1][None], outs[2][None], *outs[3:])


def solution(mesh):
    dims = (4, 4, 8)
    return on_torus(Mesh(mesh.devices.reshape(*dims, 2), ("y", "x", "z", "c")), dims)


def on_torus(torus, dims):
    sp, tp = ("y", "x"), ("z", "c")
    return jax.shard_map(
        functools.partial(shards, dims),
        mesh=torus,
        in_specs=(
            P(tp, sp),
            P(tp, sp),
            P(tp, sp),
            P(None, tp),
            P(tp, None),
            P(sp, tp),
            P(sp, None),
            P(sp, None),
            P(sp, tp, None),
            P(sp, tp, None),
            P(sp, tp, None),
            P(sp, tp),
        ),
        out_specs=(
            P(sp, tp, None),
            P(sp, tp, None),
            P(sp, tp, None),
            P(sp, tp),
            P(tp, sp),
            P(tp, sp),
            P(tp, sp),
            P(tp, sp),
        ),
        check_vma=False,
    )
```
